512 devices in a mesh: rep: 2 (over z_hi), fs: 32 (over z_lo, y), tp: 8 (over x, core).
Axes of the slice: x: 4, y: 8, z: 8 (z_hi: 2, z_lo: 4; z = z_hi * 4 + z_lo), core: 2. Of those that a mesh axis runs over, the one named last changes fastest.
Arguments:
- late_rows: bfloat16 [16384, 2048], P(('rep', 'fs')), parts along dimension 0, may hold values from -6 to 6
- early_rows: bfloat16 [16384, 2048], P(('rep', 'fs')), parts along dimension 0, may hold values from -6 to 6
- hidden_cot: bfloat16 [16384, 5632], P(('rep', 'fs'), 'tp'), parts along dimension 0, may hold values from -6 to 6
- gate_weight: bfloat16 [2048, 5632], P('fs', 'tp'), may hold values from -0.125 to 0.125
- up_weight: bfloat16 [2048, 5632], P('fs', 'tp'), may hold values from -0.125 to 0.125
- gate_taps: bfloat16 [3, 5632], P(None, 'tp'), may hold values from -3.5 to 3.5
- up_taps: bfloat16 [3, 5632], P(None, 'tp'), may hold values from -3.5 to 3.5
- gate_grad_sum: float32 [4096, 5632], P(('rep', 'fs'), 'tp'), parts along dimension 0, may hold values from -6 to 6
- up_grad_sum: float32 [4096, 5632], P(('rep', 'fs'), 'tp'), parts along dimension 0, may hold values from -6 to 6
- gate_taps_sum: float32 [6, 5632], P('rep', 'tp'), parts along dimension 0, may hold values from -6 to 6
- up_taps_sum: float32 [6, 5632], P('rep', 'tp'), parts along dimension 0, may hold values from -6 to 6
Outputs:
- late_hidden: bfloat16 [16384, 5632], P(('rep', 'fs'), 'tp'), parts along dimension 0
- early_grad: bfloat16 [16384, 2048], P(('rep', 'fs')), parts along dimension 0
- gate_grad_next: float32 [4096, 5632], P(('rep', 'fs'), 'tp'), parts along dimension 0
- up_grad_next: float32 [4096, 5632], P(('rep', 'fs'), 'tp'), parts along dimension 0
- gate_taps_next: float32 [6, 5632], P('rep', 'tp'), parts along dimension 0
- up_taps_next: float32 [6, 5632], P('rep', 'tp'), parts along dimension 0
The draws below stay inside these ranges and needn't reach their ends.
There are 2 independent parts, one for each index of `rep`. The reference program is written for one: setup_inputs(seed, part) draws one part's arguments, and reference() takes and returns one part's arrays. A program takes and returns all parts, laid end to end along the dimension named above; an argument that names none is the same for every part. Nothing has to cross between parts.
All inputs are finite; a program needn't handle non-finite values.
Results may differ from the reference program's by a relative error of at most 0.02.
Values may be sent and summed in bfloat16 or wider, within the bound.
No kernel may reach another device: no remote copies, remote signals or barrier semaphores. Data moves between devices by JAX's collectives and lax.ppermute only.
A program may use at most 64 MiB of HBM per device.

```python
import jax
import jax.numpy as jnp
from jax import lax

D = 2048
FF = 5632
TAPS = 3
TOK_DEV = 256
TOKENS = 8192
N_FS = 32


def strengthened(entries, stream_key, source, target, shards_of, factor):
    owner, partner = [(jnp.arange(entries.shape[position]) // (entries.shape[position] // shards_of)).reshape([-1 if axis == position else 1 for axis in range(entries.ndim)]) for position in (source, target)]
    chosen = jax.random.permutation(stream_key, shards_of)[partner]
    strong = (owner == chosen) | (owner == (partner + shards_of // 2) % shards_of)
    return jnp.where(strong, factor * entries, entries)


def levels(own_key, dims, pieces, least, high):
    def one(axis_at, parts):
        steps = jax.random.uniform(jax.random.fold_in(jax.random.fold_in(own_key, 6), axis_at), (parts,), jnp.float32, least / len(pieces), high / len(pieces))
        return jnp.repeat(jnp.exp(steps), dims[axis_at] // parts).reshape((-1,) + (1,) * (len(dims) - axis_at - 1))

    level = one(*pieces[0])
    for cut in pieces[1:]:
        level = level * one(*cut)
    return level


def bell_draw(own_key, shape, spread, bound, cuts=(), dtype=jnp.bfloat16):
    gain = levels(own_key, shape, cuts, -0.22, 0.18) if cuts else 1.0
    drawn = jax.random.normal(own_key, shape, jnp.float32) * spread * gain
    return jnp.minimum(jnp.maximum(drawn, -bound), bound).astype(dtype)


def bell_draw_with(rng, extent, width, bound, pieces, heavy, held_as=jnp.bfloat16):
    drawn = width * jax.random.normal(rng, extent, jnp.float32)
    if pieces:
        drawn = drawn * levels(rng, extent, pieces, -0.22, 0.18)
    return jnp.clip(strengthened(drawn, jax.random.fold_in(rng, 3), *heavy), -bound, bound).astype(held_as)


def setup_inputs(seed: int = 0, part: int = 0) -> dict:
    key_list = jax.random.split(jax.random.key(seed), 12)
    own_keys = jax.random.split(jax.random.fold_in(key_list[11], part), 12)
    return {
        "late_rows": bell_draw(own_keys[0], (TOKENS, D), 1.0, 6.0, ((0, 32),)),
        "early_rows": bell_draw_with(own_keys[1], (TOKENS, D), 1.0, 6.0, ((0, 32),), (0, 1, 32, 2.75)),
        "hidden_cot": bell_draw_with(own_keys[2], (TOKENS, FF), 1.0, 6.0, ((0, 32), (1, 8)), (0, 1, 32, 2.75)),
        "gate_weight": bell_draw(key_list[3], (D, FF), D ** -0.5, 0.125, ((0, 32), (1, 8))),
        "up_weight": bell_draw(key_list[4], (D, FF), D ** -0.5, 0.125, ((0, 32), (1, 8))),
        "gate_taps": bell_draw(key_list[5], (TAPS, FF), TAPS ** -0.5, 3.5, ((1, 8),)),
        "up_taps": bell_draw(key_list[6], (TAPS, FF), TAPS ** -0.5, 3.5, ((1, 8),)),
        "gate_grad_sum": bell_draw(own_keys[7], (D, FF), 1.0, 6.0, ((0, 32), (1, 8)), jnp.float32),
        "up_grad_sum": bell_draw(own_keys[8], (D, FF), 1.0, 6.0, ((0, 32), (1, 8)), jnp.float32),
        "gate_taps_sum": bell_draw(own_keys[9], (TAPS, FF), 1.0, 6.0, ((1, 8),), jnp.float32),
        "up_taps_sum": bell_draw(own_keys[10], (TAPS, FF), 1.0, 6.0, ((1, 8),), jnp.float32),
    }


def causal_mix(values, filter_taps):
    length = values.shape[-2]
    widths = [(0, 0)] * values.ndim
    widths[-2] = (2, 0)
    padded = jnp.pad(values, widths)
    return filter_taps[0] * padded[..., 0:length, :] + filter_taps[1] * padded[..., 1:length + 1, :] + filter_taps[2] * padded[..., 2:length + 2, :]

def mix_back(grads, filter_taps):
    length = grads.shape[-2]
    widths = [(0, 0)] * grads.ndim
    widths[-2] = (0, 2)
    padded = jnp.pad(grads, widths)
    return filter_taps[2] * padded[..., 0:length, :] + filter_taps[1] * padded[..., 1:length + 1, :] + filter_taps[0] * padded[..., 2:length + 2, :]

def tap_products(grads, values):
    length = values.shape[-2]
    widths = [(0, 0)] * values.ndim
    widths[-2] = (2, 0)
    padded = jnp.pad(values, widths)
    axes = tuple(range(values.ndim - 1))
    return jnp.stack([lax.optimization_barrier(jnp.sum(grads * padded[..., offset:offset + length, :], axis=axes)) for offset in range(3)])

def stored(product):
    return lax.optimization_barrier(product.astype(jnp.bfloat16)).astype(jnp.float32)

def reference(late_rows, early_rows, hidden_cot, gate_weight, up_weight, gate_taps, up_taps, gate_grad_sum, up_grad_sum, gate_taps_sum, up_taps_sum):
    rows_scale = TOKENS ** (-0.5)
    gate_filter = gate_taps.astype(jnp.float32)
    up_filter = up_taps.astype(jnp.float32)

    def project(source):
        gate_pre = stored(jnp.dot(source, gate_weight, preferred_element_type=jnp.float32))
        up_pre = stored(jnp.dot(source, up_weight, preferred_element_type=jnp.float32))
        return (gate_pre.reshape(N_FS, TOK_DEV, FF), up_pre.reshape(N_FS, TOK_DEV, FF))
    late_gate, late_up = project(late_rows)
    late_hidden = (jax.nn.gelu(causal_mix(late_gate, gate_filter), approximate=True) * causal_mix(late_up, up_filter)).astype(jnp.bfloat16).reshape(TOKENS, FF)
    early_gate, early_up = project(early_rows)
    gate_mix = causal_mix(early_gate, gate_filter)
    up_mix = causal_mix(early_up, up_filter)
    cotangent = hidden_cot.astype(jnp.float32).reshape(N_FS, TOK_DEV, FF)
    activated, gelu_back = jax.vjp(lambda mixed_value: jax.nn.gelu(mixed_value, approximate=True), gate_mix)
    d_gate_mix = gelu_back(cotangent * up_mix)[0]
    d_up_mix = cotangent * activated
    d_gate_pre = mix_back(d_gate_mix, gate_filter).astype(jnp.bfloat16)
    d_up_pre = mix_back(d_up_mix, up_filter).astype(jnp.bfloat16)
    gate_taps_next = gate_taps_sum + rows_scale * tap_products(d_gate_mix, early_gate)
    up_taps_next = up_taps_sum + rows_scale * tap_products(d_up_mix, early_up)
    flat_gate = d_gate_pre.reshape(TOKENS, FF)
    flat_up = d_up_pre.reshape(TOKENS, FF)
    early_grad = (jnp.dot(flat_gate, gate_weight.T, preferred_element_type=jnp.float32) + jnp.dot(flat_up, up_weight.T, preferred_element_type=jnp.float32)).astype(jnp.bfloat16)
    both_grads = jnp.concatenate([d_gate_pre, d_up_pre], axis=-1)
    blocks = early_rows.reshape(N_FS, TOK_DEV, D)

    def add_device(total, pair):
        block_rows, block_grads = pair
        term = (jnp.dot(block_rows.T, block_grads, preferred_element_type=jnp.float32) * rows_scale).astype(jnp.bfloat16)
        term = lax.optimization_barrier(term)
        return (total + term.astype(jnp.float32), None)
    summed = lax.scan(add_device, jnp.zeros((D, 2 * FF), jnp.float32), (blocks, both_grads))[0]
    return (late_hidden, early_grad, gate_grad_sum + summed[:, :FF], up_grad_sum + summed[:, FF:], gate_taps_next, up_taps_next)
```

```python
import jax
import jax.numpy as jnp
from jax import lax
from jax.sharding import Mesh
from jax.sharding import PartitionSpec as P

Z_ALL = ("rep", "zp", "zb")
FS = ("zp", "zb", "y")
REP_FS = ("rep", "zp", "zb", "y")
TP = ("x", "c")

contract_last = (((1,), (1,)), ((), ()))
contract_first = (((0,), (0,)), ((), ()))


def shifted(values, axis, by):
    size = lax.axis_size(axis)
    return lax.ppermute(values, axis, [(k, (k + by) % size) for k in range(size)])


def swapped(values, axis):
    return lax.ppermute(values, axis, [(0, 1), (1, 0)])


def pick(flag, first, second):
    return jnp.where(flag, first, second)


def causal_mix(values, filter_taps):
    length = values.shape[-2]
    widths = [(0, 0)] * values.ndim
    widths[-2] = (2, 0)
    padded = jnp.pad(values, widths)
    return (
        filter_taps[0] * padded[..., 0:length, :]
        + filter_taps[1] * padded[..., 1 : length + 1, :]
        + filter_taps[2] * padded[..., 2 : length + 2, :]
    )


def mix_back(grads, filter_taps):
    length = grads.shape[-2]
    widths = [(0, 0)] * grads.ndim
    widths[-2] = (0, 2)
    padded = jnp.pad(grads, widths)
    return (
        filter_taps[2] * padded[..., 0:length, :]
        + filter_taps[1] * padded[..., 1 : length + 1, :]
        + filter_taps[0] * padded[..., 2 : length + 2, :]
    )


def tap_products(grads, values):
    length = values.shape[-2]
    widths = [(0, 0)] * values.ndim
    widths[-2] = (2, 0)
    padded = jnp.pad(values, widths)
    axes = tuple(range(values.ndim - 1))
    return jnp.stack(
        [
            jnp.sum(grads * padded[..., offset : offset + length, :], axis=axes)
            for offset in range(3)
        ]
    )


def stored(product):
    return lax.optimization_barrier(product.astype(jnp.bfloat16)).astype(jnp.float32)


def rolled(blocks, by):
    size = blocks.shape[0]
    twice = jnp.concatenate([blocks, blocks], axis=0)
    return lax.dynamic_slice_in_dim(twice, (size - by) % size, size, 0)


def gathered_ring(block, axis):
    size = lax.axis_size(axis)
    half = size // 2
    cut = block.shape[0] // 2
    from_below, from_above = [block], [block]
    for step in range(1, half):
        from_below.append(shifted(from_below[-1], axis, 1))
        from_above.append(shifted(from_above[-1], axis, -1))
    far = jnp.concatenate(
        [shifted(from_below[-1][:cut], axis, 1), shifted(from_above[-1][cut:], axis, -1)]
    )
    return jnp.stack(from_above + [far] + from_below[:0:-1])


def summed_ring(block_of, axis):
    size = lax.axis_size(axis)
    half = size // 2
    far = block_of(half)
    cut = far.shape[0] // 2
    up = shifted(far[:cut], axis, 1)
    down = shifted(far[cut:], axis, -1)
    for step in range(half - 1, 0, -1):
        above, below = block_of(step), block_of(-step)
        if step == half - 1:
            above = jnp.concatenate([above[:cut] + up, above[cut:]])
            below = jnp.concatenate([below[:cut], below[cut:] + down])
        else:
            above = above + up
            below = below + down
        up = shifted(above, axis, 1)
        down = shifted(below, axis, -1)
    wide = jnp.float32
    return block_of(0).astype(wide) + up.astype(wide) + down.astype(wide)


def per_device(
    late_rows,
    early_rows,
    hidden_cot,
    gate_weight,
    up_weight,
    gate_taps,
    up_taps,
    gate_grad_sum,
    up_grad_sum,
    gate_taps_sum,
    up_taps_sum,
):
    row_count, depth = late_rows.shape
    shard_rows, width_local = gate_weight.shape
    width = width_local // 2
    n_z = lax.axis_size("zp") * lax.axis_size("zb")
    n_y = lax.axis_size("y")
    n_x = lax.axis_size("x")
    zb = lax.axis_index("zb")
    z = lax.axis_index("zp") * 2 + zb
    y = lax.axis_index("y")
    first_z = zb == 0
    first_c = lax.axis_index("c") == 0
    rows_scale = (row_count * n_z * n_y) ** (-0.5)

    def halves(array):
        low, high = array[..., :width], array[..., width:]
        return pick(first_z, low, high), pick(first_z, high, low)

    def columns_joined(mine, other):
        return pick(
            first_z,
            jnp.concatenate([mine, other], axis=-1),
            jnp.concatenate([other, mine], axis=-1),
        )

    def partner_rows(rows):
        cut = row_count // 2
        sent = pick(first_c, rows[:cut], rows[cut:])
        here = swapped(sent, "zb")
        there = swapped(here, "c")
        return jnp.concatenate([pick(first_c, here, there), pick(first_c, there, here)])

    gate_mine, gate_other = halves(gate_weight)
    up_mine, up_other = halves(up_weight)
    weight_mine = jnp.concatenate([gate_mine, up_mine], axis=1)
    weight_other = jnp.concatenate([gate_other, up_other], axis=1)
    next_one = shifted(weight_other, Z_ALL, -1)
    previous_one = shifted(weight_other, Z_ALL, 1)
    opposite = shifted(weight_mine, Z_ALL, -2)
    block = rolled(jnp.stack([weight_mine, next_one, opposite, previous_one]), z)
    early_pair = jnp.concatenate([early_rows, partner_rows(early_rows)])
    cot_mine, cot_other = halves(hidden_cot)
    cotangent = jnp.stack([cot_mine, swapped(cot_other, "zb")]).astype(jnp.float32)
    late_pair = jnp.concatenate([late_rows, partner_rows(late_rows)])
    gate_filter = halves(gate_taps)[0].astype(jnp.float32)
    up_filter = halves(up_taps)[0].astype(jnp.float32)

    weight = rolled(gathered_ring(block, "y"), y)
    weight = weight.transpose(1, 0, 2, 3).reshape(depth, 2 * width)

    def project(rows):
        product = stored(jnp.dot(rows, weight, preferred_element_type=jnp.float32))
        product = product.reshape(2, row_count, 2 * width)
        return product[..., :width], product[..., width:]

    early_gate, early_up = project(early_pair)
    gate_mix = causal_mix(early_gate, gate_filter)
    up_mix = causal_mix(early_up, up_filter)
    activated, gelu_back = jax.vjp(
        lambda mixed_value: jax.nn.gelu(mixed_value, approximate=True), gate_mix
    )
    d_gate_mix = gelu_back(cotangent * up_mix)[0]
    d_up_mix = cotangent * activated
    d_gate_pre = mix_back(d_gate_mix, gate_filter).astype(jnp.bfloat16)
    d_up_pre = mix_back(d_up_mix, up_filter).astype(jnp.bfloat16)
    both_grads = jnp.concatenate([d_gate_pre, d_up_pre], axis=-1)
    both_grads = both_grads.reshape(2 * row_count, 2 * width)

    terms = (
        lax.dot_general(
            early_pair, both_grads, contract_first, preferred_element_type=jnp.float32
        )
        * rows_scale
    ).astype(jnp.bfloat16)
    terms = terms.reshape(n_z, n_y, shard_rows, 2 * width)

    def terms_for(offset):
        at = (y + offset + n_y) % n_y
        return lax.dynamic_index_in_dim(terms, at, 1, keepdims=False)

    reduced = summed_ring(terms_for, "y").astype(jnp.bfloat16)
    pieces = lax.all_to_all(reduced, ("zp", "zb"), 0, 0, tiled=True)
    pieces = pieces.reshape(2, 2, shard_rows, 2 * width).astype(jnp.float32)
    pieces = jnp.sum(pieces, axis=0)
    gate_sum = jnp.concatenate([pieces[0, :, :width], pieces[1, :, :width]], axis=1)
    up_sum = jnp.concatenate([pieces[0, :, width:], pieces[1, :, width:]], axis=1)

    partial = lax.dot_general(
        both_grads, weight, contract_last, preferred_element_type=jnp.float32
    )
    cut = depth // 2
    kept = pick(first_c, partial[:, :cut], partial[:, cut:])
    given = pick(first_c, partial[:, cut:], partial[:, :cut]).astype(jnp.bfloat16)
    chip = (kept + swapped(given, "c").astype(jnp.float32)).astype(jnp.bfloat16)
    chip = chip.reshape(2, n_x, row_count // n_x, cut)
    chip = jnp.stack([pick(first_z, chip[0], chip[1]), pick(first_z, chip[1], chip[0])])
    spread = lax.all_to_all(
        chip.reshape(2 * n_x, row_count // n_x, cut), ("zb", "x"), 0, 0, tiled=True
    )
    own = jnp.sum(spread.astype(jnp.float32), axis=0).astype(jnp.bfloat16)
    copies = jnp.broadcast_to(own[None], (2 * n_x, *own.shape))
    finished = lax.all_to_all(copies, TP, 0, 0, tiled=True)
    finished = finished.reshape(n_x, 2, row_count // n_x, cut)
    early_grad = finished.transpose(0, 2, 1, 3).reshape(row_count, depth)

    taps = rows_scale * jnp.concatenate(
        [tap_products(d_gate_mix, early_gate), tap_products(d_up_mix, early_up)], axis=0
    )
    n_fs = n_z * n_y
    all_taps = lax.all_to_all(
        jnp.broadcast_to(taps.reshape(1, -1), (n_fs, taps.size)), FS, 0, 0, tiled=True
    )
    all_taps = jnp.sum(all_taps.reshape(n_z // 2, 2, n_y, taps.size), axis=(0, 2))
    all_taps = all_taps.reshape(2, 6, width).transpose(1, 0, 2).reshape(6, width_local)

    late_gate, late_up = project(late_pair)
    late = (
        jax.nn.gelu(causal_mix(late_gate, gate_filter), approximate=True)
        * causal_mix(late_up, up_filter)
    ).astype(jnp.bfloat16)
    late_hidden = columns_joined(late[0], swapped(late[1], "zb"))
    return (
        late_hidden,
        early_grad,
        gate_grad_sum + gate_sum,
        up_grad_sum + up_sum,
        gate_taps_sum + all_taps[:3],
        up_taps_sum + all_taps[3:],
    )


def solution(mesh):
    split = Mesh(
        mesh.devices.reshape(mesh.shape["rep"], 2, 2, 8, 4, 2),
        ("rep", "zp", "zb", "y", "x", "c"),
    )
    placed = (
        P(REP_FS, None),
        P(REP_FS, None),
        P(REP_FS, TP),
        P(FS, TP),
        P(FS, TP),
        P(None, TP),
        P(None, TP),
        P(REP_FS, TP),
        P(REP_FS, TP),
        P("rep", TP),
        P("rep", TP),
    )
    return jax.shard_map(
        per_device,
        mesh=split,
        in_specs=placed,
        out_specs=(
            P(REP_FS, TP),
            P(REP_FS, None),
            P(REP_FS, TP),
            P(REP_FS, TP),
            P("rep", TP),
            P("rep", TP),
        ),
        check_vma=False,
    )
```

```python
import jax
import jax.numpy as jnp
from jax import lax
from jax.sharding import Mesh
from jax.sharding import PartitionSpec as P

Z = ("zp", "zb")
FS = ("zp", "zb", "y")
REP_FS = ("rep", "zp", "zb", "y")
TP = ("x", "c")

contract_last = (((1,), (1,)), ((), ()))
contract_first = (((0,), (0,)), ((), ()))


def swapped(values, axis):
    return lax.ppermute(values, axis, [(0, 1), (1, 0)])


def pick(flag, first, second):
    return jnp.where(flag, first, second)


def causal_mix(values, filter_taps):
    length = values.shape[-2]
    widths = [(0, 0)] * values.ndim
    widths[-2] = (2, 0)
    padded = jnp.pad(values, widths)
    return (
        filter_taps[0] * padded[..., 0:length, :]
        + filter_taps[1] * padded[..., 1 : length + 1, :]
        + filter_taps[2] * padded[..., 2 : length + 2, :]
    )


def mix_back(grads, filter_taps):
    length = grads.shape[-2]
    widths = [(0, 0)] * grads.ndim
    widths[-2] = (0, 2)
    padded = jnp.pad(grads, widths)
    return (
        filter_taps[2] * padded[..., 0:length, :]
        + filter_taps[1] * padded[..., 1 : length + 1, :]
        + filter_taps[0] * padded[..., 2 : length + 2, :]
    )


def tap_products(grads, values):
    length = values.shape[-2]
    widths = [(0, 0)] * values.ndim
    widths[-2] = (2, 0)
    padded = jnp.pad(values, widths)
    axes = tuple(range(values.ndim - 1))
    return jnp.stack(
        [
            jnp.sum(grads * padded[..., offset : offset + length, :], axis=axes)
            for offset in range(3)
        ]
    )


def stored(product):
    return lax.optimization_barrier(product.astype(jnp.bfloat16)).astype(jnp.float32)


def per_device(
    late_rows,
    early_rows,
    hidden_cot,
    gate_weight,
    up_weight,
    gate_taps,
    up_taps,
    gate_grad_sum,
    up_grad_sum,
    gate_taps_sum,
    up_taps_sum,
):
    row_count, depth = late_rows.shape
    shard_rows, width_local = gate_weight.shape
    width = width_local // 2
    n_z = lax.axis_size("zp") * lax.axis_size("zb")
    n_y = lax.axis_size("y")
    n_x = lax.axis_size("x")
    zb = lax.axis_index("zb")
    first_z = zb == 0
    first_c = lax.axis_index("c") == 0
    rows_scale = (row_count * n_z * n_y) ** (-0.5)

    def halves(array):
        low, high = array[..., :width], array[..., width:]
        return pick(first_z, low, high), pick(first_z, high, low)

    def columns_joined(mine, other):
        return pick(
            first_z,
            jnp.concatenate([mine, other], axis=-1),
            jnp.concatenate([other, mine], axis=-1),
        )

    def own_and_partner(late, early):
        cut = row_count // 2
        sent = jnp.concatenate(
            [pick(first_c, rows[:cut], rows[cut:]) for rows in (early, late)]
        )
        here = swapped(sent, "zb")
        there = swapped(here, "c")
        low, high = pick(first_c, here, there), pick(first_c, there, here)
        return (
            jnp.concatenate([late, low[cut:], high[cut:]]),
            jnp.concatenate([early, low[:cut], high[:cut]]),
        )

    gate_mine, gate_other = halves(gate_weight)
    up_mine, up_other = halves(up_weight)
    weight_mine = jnp.concatenate([gate_mine, up_mine], axis=1)
    weight_other = jnp.concatenate([gate_other, up_other], axis=1)
    for_z = jnp.stack(
        [pick(first_z, weight_mine, weight_other), pick(first_z, weight_other, weight_mine)] * 2
    )
    block = lax.all_to_all(for_z, Z, 0, 0, tiled=True)
    late_pair, early_pair = own_and_partner(late_rows, early_rows)
    cot_mine, cot_other = halves(hidden_cot)
    cotangent = jnp.stack([cot_mine, swapped(cot_other, "zb")]).astype(jnp.float32)
    gate_filter = halves(gate_taps)[0].astype(jnp.float32)
    up_filter = halves(up_taps)[0].astype(jnp.float32)

    copies = jnp.broadcast_to(block[None], (n_y, *block.shape))
    weight = lax.all_to_all(copies, "y", 0, 0, tiled=True)
    weight = weight.transpose(1, 0, 2, 3).reshape(depth, 2 * width)

    def project(rows):
        product = stored(jnp.dot(rows, weight, preferred_element_type=jnp.float32))
        product = product.reshape(2, row_count, 2 * width)
        return product[..., :width], product[..., width:]

    early_gate, early_up = project(early_pair)
    gate_mix = causal_mix(early_gate, gate_filter)
    up_mix = causal_mix(early_up, up_filter)
    activated, gelu_back = jax.vjp(
        lambda mixed_value: jax.nn.gelu(mixed_value, approximate=True), gate_mix
    )
    d_gate_mix = gelu_back(cotangent * up_mix)[0]
    d_up_mix = cotangent * activated
    d_gate_pre = mix_back(d_gate_mix, gate_filter).astype(jnp.bfloat16)
    d_up_pre = mix_back(d_up_mix, up_filter).astype(jnp.bfloat16)
    both_grads = jnp.concatenate([d_gate_pre, d_up_pre], axis=-1)
    both_grads = both_grads.reshape(2 * row_count, 2 * width)

    terms = (
        lax.dot_general(
            early_pair, both_grads, contract_first, preferred_element_type=jnp.float32
        )
        * rows_scale
    ).astype(jnp.bfloat16)
    terms = terms.reshape(n_z, n_y, shard_rows, 2 * width)

    terms = lax.all_to_all(terms.transpose(1, 0, 2, 3), "y", 0, 0, tiled=True)
    reduced = jnp.sum(terms.astype(jnp.float32), axis=0).astype(jnp.bfloat16)
    pieces = lax.all_to_all(reduced, Z, 0, 0, tiled=True)
    pieces = pieces.reshape(2, 2, shard_rows, 2 * width).astype(jnp.float32)
    pieces = jnp.sum(pieces, axis=0)
    gate_sum = jnp.concatenate([pieces[0, :, :width], pieces[1, :, :width]], axis=1)
    up_sum = jnp.concatenate([pieces[0, :, width:], pieces[1, :, width:]], axis=1)

    partial = lax.dot_general(
        both_grads, weight, contract_last, preferred_element_type=jnp.float32
    )
    cut = depth // 2
    kept = pick(first_c, partial[:, :cut], partial[:, cut:])
    given = pick(first_c, partial[:, cut:], partial[:, :cut]).astype(jnp.bfloat16)
    chip = (kept + swapped(given, "c").astype(jnp.float32)).astype(jnp.bfloat16)
    chip = chip.reshape(2, n_x, row_count // n_x, cut)
    chip = jnp.stack([pick(first_z, chip[0], chip[1]), pick(first_z, chip[1], chip[0])])
    spread = lax.all_to_all(
        chip.reshape(2 * n_x, row_count // n_x, cut), ("zb", "x"), 0, 0, tiled=True
    )
    own = jnp.sum(spread.astype(jnp.float32), axis=0).astype(jnp.bfloat16)
    copies = jnp.broadcast_to(own[None], (2 * n_x, *own.shape))
    finished = lax.all_to_all(copies, TP, 0, 0, tiled=True)
    finished = finished.reshape(n_x, 2, row_count // n_x, cut)
    early_grad = finished.transpose(0, 2, 1, 3).reshape(row_count, depth)

    taps = rows_scale * jnp.concatenate(
        [tap_products(d_gate_mix, early_gate), tap_products(d_up_mix, early_up)], axis=0
    )
    n_fs = n_z * n_y
    all_taps = lax.all_to_all(
        jnp.broadcast_to(taps.reshape(1, -1), (n_fs, taps.size)), FS, 0, 0, tiled=True
    )
    all_taps = jnp.sum(all_taps.reshape(n_z // 2, 2, n_y, taps.size), axis=(0, 2))
    all_taps = all_taps.reshape(2, 6, width).transpose(1, 0, 2).reshape(6, width_local)

    late_gate, late_up = project(late_pair)
    late = (
        jax.nn.gelu(causal_mix(late_gate, gate_filter), approximate=True)
        * causal_mix(late_up, up_filter)
    ).astype(jnp.bfloat16)
    late_hidden = columns_joined(late[0], swapped(late[1], "zb"))
    return (
        late_hidden,
        early_grad,
        gate_grad_sum + gate_sum,
        up_grad_sum + up_sum,
        gate_taps_sum + all_taps[:3],
        up_taps_sum + all_taps[3:],
    )


def solution(mesh):
    split = Mesh(
        mesh.devices.reshape(mesh.shape["rep"], 2, 2, 8, 4, 2),
        ("rep", "zp", "zb", "y", "x", "c"),
    )
    placed = (
        P(REP_FS, None),
        P(REP_FS, None),
        P(REP_FS, TP),
        P(FS, TP),
        P(FS, TP),
        P(None, TP),
        P(None, TP),
        P(REP_FS, TP),
        P(REP_FS, TP),
        P("rep", TP),
        P("rep", TP),
    )
    return jax.shard_map(
        per_device,
        mesh=split,
        in_specs=placed,
        out_specs=(
            P(REP_FS, TP),
            P(REP_FS, None),
            P(REP_FS, TP),
            P(REP_FS, TP),
            P("rep", TP),
            P("rep", TP),
        ),
        check_vma=False,
    )
```

```python
import jax
import jax.numpy as jnp
from jax import lax
from jax.sharding import Mesh
from jax.sharding import PartitionSpec as P

Z = ("zp", "zb")
FS = ("zp", "zb", "y")
REP_FS = ("rep", "zp", "zb", "y")
TP = ("x", "c")

contract_last = (((1,), (1,)), ((), ()))
contract_first = (((0,), (0,)), ((), ()))


def swapped(values, axis):
    return lax.ppermute(values, axis, [(0, 1), (1, 0)])


def pick(flag, first, second):
    return jnp.where(flag, first, second)


def causal_mix(values, filter_taps):
    length = values.shape[-2]
    widths = [(0, 0)] * values.ndim
    widths[-2] = (2, 0)
    padded = jnp.pad(values, widths)
    return (
        filter_taps[0] * padded[..., 0:length, :]
        + filter_taps[1] * padded[..., 1 : length + 1, :]
        + filter_taps[2] * padded[..., 2 : length + 2, :]
    )


def mix_back(grads, filter_taps):
    length = grads.shape[-2]
    widths = [(0, 0)] * grads.ndim
    widths[-2] = (0, 2)
    padded = jnp.pad(grads, widths)
    return (
        filter_taps[2] * padded[..., 0:length, :]
        + filter_taps[1] * padded[..., 1 : length + 1, :]
        + filter_taps[0] * padded[..., 2 : length + 2, :]
    )


def tap_products(grads, values):
    length = values.shape[-2]
    widths = [(0, 0)] * values.ndim
    widths[-2] = (2, 0)
    padded = jnp.pad(values, widths)
    axes = tuple(range(values.ndim - 1))
    return jnp.stack(
        [
            jnp.sum(grads * padded[..., offset : offset + length, :], axis=axes)
            for offset in range(3)
        ]
    )


def stored(product):
    return lax.optimization_barrier(product.astype(jnp.bfloat16)).astype(jnp.float32)


def per_device(
    late_rows,
    early_rows,
    hidden_cot,
    gate_weight,
    up_weight,
    gate_taps,
    up_taps,
    gate_grad_sum,
    up_grad_sum,
    gate_taps_sum,
    up_taps_sum,
):
    row_count, depth = late_rows.shape
    shard_rows, width_local = gate_weight.shape
    width = width_local // 2
    wide = -(-width // 128) * 128
    n_z = lax.axis_size("zp") * lax.axis_size("zb")
    n_y = lax.axis_size("y")
    n_x = lax.axis_size("x")
    zb = lax.axis_index("zb")
    first_z = zb == 0
    first_c = lax.axis_index("c") == 0
    rows_scale = (row_count * n_z * n_y) ** (-0.5)

    def widened(array):
        edges = [(0, 0)] * (array.ndim - 1)
        return jnp.pad(array, edges + [(0, wide - width)])

    def halves(array):
        low, high = widened(array[..., :width]), widened(array[..., width:])
        return pick(first_z, low, high), pick(first_z, high, low)

    def columns_joined(mine, other):
        return pick(
            first_z,
            jnp.concatenate([mine, other], axis=-1),
            jnp.concatenate([other, mine], axis=-1),
        )

    def own_and_partner(late, early):
        cut = row_count // 2
        sent = jnp.concatenate(
            [pick(first_c, rows[:cut], rows[cut:]) for rows in (early, late)]
        )
        here = swapped(sent, "zb")
        there = swapped(here, "c")
        low, high = pick(first_c, here, there), pick(first_c, there, here)
        return (
            jnp.concatenate([late, low[cut:], high[cut:]]),
            jnp.concatenate([early, low[:cut], high[:cut]]),
        )

    gate_mine, gate_other = halves(gate_weight)
    up_mine, up_other = halves(up_weight)
    weight_mine = jnp.concatenate([gate_mine, up_mine], axis=1)
    weight_other = jnp.concatenate([gate_other, up_other], axis=1)
    for_z = jnp.stack(
        [pick(first_z, weight_mine, weight_other), pick(first_z, weight_other, weight_mine)] * 2
    )
    block = lax.all_to_all(for_z, Z, 0, 0, tiled=True)
    late_pair, early_pair = own_and_partner(late_rows, early_rows)
    cot_mine, cot_other = halves(hidden_cot)
    cotangent = jnp.stack([cot_mine, swapped(cot_other, "zb")]).astype(jnp.float32)
    gate_filter = halves(gate_taps)[0].astype(jnp.float32)
    up_filter = halves(up_taps)[0].astype(jnp.float32)

    block = block.reshape(n_z * shard_rows, 2 * wide)
    weight = lax.all_gather(block, "y").reshape(n_y, n_z, shard_rows, 2 * wide)
    weight = weight.transpose(1, 0, 2, 3).reshape(depth, 2 * wide)

    def project(rows):
        product = stored(jnp.dot(rows, weight, preferred_element_type=jnp.float32))
        product = product.reshape(2, row_count, 2 * wide)
        return product[..., :wide], product[..., wide:]

    early_gate, early_up = project(early_pair)
    gate_mix = causal_mix(early_gate, gate_filter)
    up_mix = causal_mix(early_up, up_filter)
    activated, gelu_back = jax.vjp(
        lambda mixed_value: jax.nn.gelu(mixed_value, approximate=True), gate_mix
    )
    d_gate_mix = gelu_back(cotangent * up_mix)[0]
    d_up_mix = cotangent * activated
    d_gate_pre = mix_back(d_gate_mix, gate_filter).astype(jnp.bfloat16)
    d_up_pre = mix_back(d_up_mix, up_filter).astype(jnp.bfloat16)
    both_grads = jnp.concatenate([d_gate_pre, d_up_pre], axis=-1)
    both_grads = both_grads.reshape(2 * row_count, 2 * wide)

    terms = (
        lax.dot_general(
            early_pair, both_grads, contract_first, preferred_element_type=jnp.float32
        )
        * rows_scale
    ).astype(jnp.bfloat16)
    terms = terms.reshape(n_z, n_y, shard_rows, 2 * wide)

    terms = terms.transpose(1, 0, 2, 3).reshape(depth, 2 * wide)
    reduced = lax.psum_scatter(terms, "y", scatter_dimension=0, tiled=True)
    reduced = reduced.reshape(n_z, shard_rows, 2 * wide)
    pieces = lax.all_to_all(reduced, Z, 0, 0, tiled=True)
    pieces = pieces.reshape(2, 2, shard_rows, 2 * wide).astype(jnp.float32)
    pieces = jnp.sum(pieces, axis=0)
    gate_sum = jnp.concatenate([pieces[0, :, :width], pieces[1, :, :width]], axis=1)
    up_sum = jnp.concatenate([pieces[0, :, wide : wide + width], pieces[1, :, wide : wide + width]], axis=1)

    partial = lax.dot_general(
        both_grads, weight, contract_last, preferred_element_type=jnp.float32
    )
    cut = depth // 2
    kept = pick(first_c, partial[:, :cut], partial[:, cut:])
    given = pick(first_c, partial[:, cut:], partial[:, :cut]).astype(jnp.bfloat16)
    chip = (kept + swapped(given, "c").astype(jnp.float32)).astype(jnp.bfloat16)
    chip = chip.reshape(2, n_x, row_count // n_x, cut)
    chip = jnp.stack([pick(first_z, chip[0], chip[1]), pick(first_z, chip[1], chip[0])])
    spread = lax.all_to_all(
        chip.reshape(2 * n_x, row_count // n_x, cut), ("zb", "x"), 0, 0, tiled=True
    )
    own = jnp.sum(spread.astype(jnp.float32), axis=0).astype(jnp.bfloat16)
    copies = jnp.broadcast_to(own[None], (2 * n_x, *own.shape))
    finished = lax.all_to_all(copies, TP, 0, 0, tiled=True)
    finished = finished.reshape(n_x, 2, row_count // n_x, cut)
    early_grad = finished.transpose(0, 2, 1, 3).reshape(row_count, depth)

    taps = rows_scale * jnp.concatenate(
        [tap_products(d_gate_mix, early_gate), tap_products(d_up_mix, early_up)], axis=0
    )
    n_fs = n_z * n_y
    all_taps = lax.all_to_all(
        jnp.broadcast_to(taps.reshape(1, -1), (n_fs, taps.size)), FS, 0, 0, tiled=True
    )
    all_taps = jnp.sum(all_taps.reshape(n_z // 2, 2, n_y, taps.size), axis=(0, 2))
    all_taps = all_taps.reshape(2, 6, wide)[..., :width].transpose(1, 0, 2).reshape(6, width_local)

    late_gate, late_up = project(late_pair)
    late = (
        jax.nn.gelu(causal_mix(late_gate, gate_filter), approximate=True)
        * causal_mix(late_up, up_filter)
    ).astype(jnp.bfloat16)
    late_hidden = columns_joined(late[0][:, :width], swapped(late[1], "zb")[:, :width])
    return (
        late_hidden,
        early_grad,
        gate_grad_sum + gate_sum,
        up_grad_sum + up_sum,
        gate_taps_sum + all_taps[:3],
        up_taps_sum + all_taps[3:],
    )


def solution(mesh):
    split = Mesh(
        mesh.devices.reshape(mesh.shape["rep"], 2, 2, 8, 4, 2),
        ("rep", "zp", "zb", "y", "x", "c"),
    )
    placed = (
        P(REP_FS, None),
        P(REP_FS, None),
        P(REP_FS, TP),
        P(FS, TP),
        P(FS, TP),
        P(None, TP),
        P(None, TP),
        P(REP_FS, TP),
        P(REP_FS, TP),
        P("rep", TP),
        P("rep", TP),
    )
    return jax.shard_map(
        per_device,
        mesh=split,
        in_specs=placed,
        out_specs=(
            P(REP_FS, TP),
            P(REP_FS, None),
            P(REP_FS, TP),
            P(REP_FS, TP),
            P("rep", TP),
            P("rep", TP),
        ),
        check_vma=False,
    )
```

```python
import functools
import math

import jax
import jax.numpy as jnp
from jax import lax
from jax.experimental import pallas as pl
from jax.experimental.pallas import tpu as pltpu
from jax.sharding import Mesh
from jax.sharding import PartitionSpec as P

Z = ("zp", "zb")
FS = ("zp", "zb", "y")
REP_FS = ("rep", "zp", "zb", "y")
TP = ("x", "c")

contract_last = (((1,), (1,)), ((), ()))
contract_first = (((0,), (0,)), ((), ()))


def swapped(values, axis):
    return lax.ppermute(values, axis, [(0, 1), (1, 0)])


def pick(flag, first, second):
    return jnp.where(flag, first, second)


def causal_mix(values, filter_taps):
    length = values.shape[-2]
    widths = [(0, 0)] * values.ndim
    widths[-2] = (2, 0)
    padded = jnp.pad(values, widths)
    return (
        filter_taps[0] * padded[..., 0:length, :]
        + filter_taps[1] * padded[..., 1 : length + 1, :]
        + filter_taps[2] * padded[..., 2 : length + 2, :]
    )


def moved(values, by):
    length = values.shape[0]
    at = lax.broadcasted_iota(jnp.int32, values.shape, 0)
    turned = pltpu.roll(values, by % length, 0)
    inside = at >= by if by > 0 else at < length + by
    return jnp.where(inside, turned, 0.0)


def early_kernel(
    scale, gathered, own, other, cotangent, filters, weight, grads, terms, tap_sums
):
    n_y, n_z, shard_rows, columns = gathered.shape
    length, depth = own.shape
    wide = columns // 2
    span = n_y * shard_rows
    for z in range(n_z):
        for y in range(n_y):
            at = z * span + y * shard_rows
            weight[at : at + shard_rows, :] = gathered[y, z]
    first, second, third = filters[0:1, :], filters[1:2, :], filters[2:3, :]
    slope = math.sqrt(2.0 / math.pi)
    sums = [jnp.zeros((1, columns), jnp.float32) for _ in range(3)]
    for part, rows in enumerate((own, other)):
        pre = jnp.dot(rows[...], weight[...], preferred_element_type=jnp.float32)
        pre = pre.astype(jnp.bfloat16).astype(jnp.float32)
        one_back, two_back = moved(pre, 1), moved(pre, 2)
        mixed = first * two_back + second * one_back + third * pre
        gate, up = mixed[:, :wide], mixed[:, wide:]
        square = gate * gate
        bend = jnp.tanh(slope * (gate + 0.044715 * (square * gate)))
        side = 0.5 * (1.0 + bend)
        active = gate * side
        rise = side + 0.5 * gate * (1.0 - bend * bend) * (
            slope * (1.0 + (3 * 0.044715) * square)
        )
        given = cotangent[part].astype(jnp.float32)
        back = jnp.concatenate([given * up * rise, given * active], axis=1)
        for tap, source in enumerate((two_back, one_back, pre)):
            sums[tap] = sums[tap] + jnp.sum(back * source, axis=0, keepdims=True)
        full = third * back + second * moved(back, -1) + first * moved(back, -2)
        grads[part * length : (part + 1) * length, :] = full.astype(jnp.bfloat16)
    tap_sums[...] = jnp.concatenate(
        [scale * value for value in sums]
        + [jnp.zeros((tap_sums.shape[0] - 3, columns), jnp.float32)]
    )
    for z in range(n_z):
        term = sum(
            lax.dot_general(
                rows[:, z * span : (z + 1) * span],
                grads[part * length : (part + 1) * length, :],
                contract_first,
                preferred_element_type=jnp.float32,
            )
            for part, rows in enumerate((own, other))
        )
        term = (term * scale).astype(jnp.bfloat16)
        for y in range(n_y):
            terms[y, z] = term[y * shard_rows : (y + 1) * shard_rows, :]


def early_pass(scale, gathered, own, other, cotangent, filters):
    n_y, n_z, shard_rows, columns = gathered.shape
    length, depth = own.shape
    whole = pl.BlockSpec(memory_space=pltpu.VMEM)
    return pl.pallas_call(
        functools.partial(early_kernel, scale),
        out_shape=(
            jax.ShapeDtypeStruct((depth, columns), jnp.bfloat16),
            jax.ShapeDtypeStruct((2 * length, columns), jnp.bfloat16),
            jax.ShapeDtypeStruct(gathered.shape, jnp.bfloat16),
            jax.ShapeDtypeStruct((8, columns), jnp.float32),
        ),
        in_specs=[whole] * 5,
        out_specs=(whole,) * 4,
        compiler_params=pltpu.CompilerParams(vmem_limit_bytes=48 * 1024 * 1024),
        cost_estimate=pl.CostEstimate(
            flops=8 * length * depth * columns,
            bytes_accessed=6 * depth * columns + 4 * length * depth,
            transcendentals=length * columns,
        ),
        name="early_pass",
    )(gathered, own, other, cotangent, filters)


def stored(product):
    return lax.optimization_barrier(product.astype(jnp.bfloat16)).astype(jnp.float32)


def per_device(
    late_rows,
    early_rows,
    hidden_cot,
    gate_weight,
    up_weight,
    gate_taps,
    up_taps,
    gate_grad_sum,
    up_grad_sum,
    gate_taps_sum,
    up_taps_sum,
):
    row_count, depth = late_rows.shape
    shard_rows, width_local = gate_weight.shape
    width = width_local // 2
    wide = -(-width // 128) * 128
    n_z = lax.axis_size("zp") * lax.axis_size("zb")
    n_y = lax.axis_size("y")
    n_x = lax.axis_size("x")
    zb = lax.axis_index("zb")
    first_z = zb == 0
    first_c = lax.axis_index("c") == 0
    rows_scale = (row_count * n_z * n_y) ** (-0.5)

    def widened(array):
        edges = [(0, 0)] * (array.ndim - 1)
        return jnp.pad(array, edges + [(0, wide - width)])

    def halves(array):
        low, high = widened(array[..., :width]), widened(array[..., width:])
        return pick(first_z, low, high), pick(first_z, high, low)

    def columns_joined(mine, other):
        return pick(
            first_z,
            jnp.concatenate([mine, other], axis=-1),
            jnp.concatenate([other, mine], axis=-1),
        )

    def partners(late, early):
        cut = row_count // 2
        sent = jnp.concatenate(
            [pick(first_c, rows[:cut], rows[cut:]) for rows in (early, late)]
        )
        here = swapped(sent, "zb")
        there = swapped(here, "c")
        low, high = pick(first_c, here, there), pick(first_c, there, here)
        return (
            jnp.concatenate([low[cut:], high[cut:]]),
            jnp.concatenate([low[:cut], high[:cut]]),
        )

    gate_mine, gate_other = halves(gate_weight)
    up_mine, up_other = halves(up_weight)
    weight_mine = jnp.concatenate([gate_mine, up_mine], axis=1)
    weight_other = jnp.concatenate([gate_other, up_other], axis=1)
    for_z = jnp.stack(
        [pick(first_z, weight_mine, weight_other), pick(first_z, weight_other, weight_mine)] * 2
    )
    block = lax.all_to_all(for_z, Z, 0, 0, tiled=True)
    late_other, early_other = partners(late_rows, early_rows)
    cot_mine, cot_other = halves(hidden_cot)
    cotangent = jnp.stack([cot_mine, swapped(cot_other, "zb")])
    filters = jnp.concatenate([halves(gate_taps)[0], halves(up_taps)[0]], axis=1)
    filters = jnp.pad(filters.astype(jnp.float32), [(0, 5), (0, 0)])

    block = block.reshape(n_z * shard_rows, 2 * wide)
    weight = lax.all_gather(block, "y").reshape(n_y, n_z, shard_rows, 2 * wide)
    weight, both_grads, terms, taps = early_pass(
        rows_scale, weight, early_rows, early_other, cotangent, filters
    )
    terms = terms.reshape(depth, 2 * wide)
    reduced = lax.psum_scatter(terms, "y", scatter_dimension=0, tiled=True)
    reduced = reduced.reshape(n_z, shard_rows, 2 * wide)
    partial = lax.dot_general(
        both_grads, weight, contract_last, preferred_element_type=jnp.float32
    )
    cut = depth // 2
    kept = pick(first_c, partial[:, :cut], partial[:, cut:])
    given = pick(first_c, partial[:, cut:], partial[:, :cut]).astype(jnp.bfloat16)
    chip = (kept + swapped(given, "c").astype(jnp.float32)).astype(jnp.bfloat16)
    chip = chip.reshape(2, n_x, row_count // n_x, cut)
    chip = jnp.stack([pick(first_z, chip[0], chip[1]), pick(first_z, chip[1], chip[0])])
    spread = lax.all_to_all(
        chip.reshape(2 * n_x, row_count // n_x, cut), ("zb", "x"), 0, 0, tiled=True
    )
    own = jnp.sum(spread.astype(jnp.float32), axis=0).astype(jnp.bfloat16)
    copies = jnp.broadcast_to(own[None], (2 * n_x, *own.shape))
    finished = lax.all_to_all(copies, TP, 0, 0, tiled=True)
    for step in (1, 2, 4):
        taps = taps + lax.ppermute(taps, "y", [(k, k ^ step) for k in range(n_y)])
    taps = taps + swapped(taps, "zp")
    gate_taps_mine, up_taps_mine = taps[:3, :width], taps[:3, wide : wide + width]
    taps = swapped(taps, "zb")
    gate_tap_sums = columns_joined(gate_taps_mine, taps[:3, :width])
    up_tap_sums = columns_joined(up_taps_mine, taps[:3, wide : wide + width])

    product = [
        stored(jnp.dot(rows, weight, preferred_element_type=jnp.float32))
        for rows in (late_rows, late_other)
    ]
    mixed = [causal_mix(values, filters) for values in product]
    late = [
        (jax.nn.gelu(values[:, :wide], approximate=True) * values[:, wide:]).astype(
            jnp.bfloat16
        )
        for values in mixed
    ]
    late_hidden = columns_joined(late[0][:, :width], swapped(late[1], "zb")[:, :width])

    reduced, finished = lax.optimization_barrier((reduced, finished))
    pieces = lax.all_to_all(reduced, Z, 0, 0, tiled=True)
    pieces = pieces.reshape(2, 2, shard_rows, 2 * wide).astype(jnp.float32)
    pieces = jnp.sum(pieces, axis=0)
    gate_sum = jnp.concatenate([pieces[0, :, :width], pieces[1, :, :width]], axis=1)
    up_sum = jnp.concatenate([pieces[0, :, wide : wide + width], pieces[1, :, wide : wide + width]], axis=1)

    finished = finished.reshape(n_x, 2, row_count // n_x, cut)
    early_grad = finished.transpose(0, 2, 1, 3).reshape(row_count, depth)
    return (
        late_hidden,
        early_grad,
        gate_grad_sum + gate_sum,
        up_grad_sum + up_sum,
        gate_taps_sum + gate_tap_sums,
        up_taps_sum + up_tap_sums,
    )


def solution(mesh):
    split = Mesh(
        mesh.devices.reshape(mesh.shape["rep"], 2, 2, 8, 4, 2),
        ("rep", "zp", "zb", "y", "x", "c"),
    )
    placed = (
        P(REP_FS, None),
        P(REP_FS, None),
        P(REP_FS, TP),
        P(FS, TP),
        P(FS, TP),
        P(None, TP),
        P(None, TP),
        P(REP_FS, TP),
        P(REP_FS, TP),
        P("rep", TP),
        P("rep", TP),
    )
    return jax.shard_map(
        per_device,
        mesh=split,
        in_specs=placed,
        out_specs=(
            P(REP_FS, TP),
            P(REP_FS, None),
            P(REP_FS, TP),
            P(REP_FS, TP),
            P("rep", TP),
            P("rep", TP),
        ),
        check_vma=False,
    )
```

```python
import functools
import math

import jax
import jax.numpy as jnp
from jax import lax
from jax.experimental import pallas as pl
from jax.experimental.pallas import tpu as pltpu
from jax.sharding import Mesh
from jax.sharding import PartitionSpec as P

Z = ("zp", "zb")
FS = ("zp", "zb", "y")
REP_FS = ("rep", "zp", "zb", "y")
TP = ("x", "c")

contract_last = (((1,), (1,)), ((), ()))
contract_first = (((0,), (0,)), ((), ()))


def swapped(values, axis):
    return lax.ppermute(values, axis, [(0, 1), (1, 0)])


def pick(flag, first, second):
    return jnp.where(flag, first, second)


def causal_mix(values, filter_taps):
    length = values.shape[-2]
    widths = [(0, 0)] * values.ndim
    widths[-2] = (2, 0)
    padded = jnp.pad(values, widths)
    return (
        filter_taps[0] * padded[..., 0:length, :]
        + filter_taps[1] * padded[..., 1 : length + 1, :]
        + filter_taps[2] * padded[..., 2 : length + 2, :]
    )


def moved(values, by):
    length = values.shape[0]
    at = lax.broadcasted_iota(jnp.int32, values.shape, 0)
    turned = pltpu.roll(values, by % length, 0)
    inside = at >= by if by > 0 else at < length + by
    return jnp.where(inside, turned, 0.0)


def early_kernel(
    scale,
    gathered,
    own,
    other,
    cotangent,
    filters,
    weight_out,
    grads_out,
    terms_out,
    tap_sums,
    weight,
    grads,
    terms,
    in_sems,
    out_sems,
):
    n_y, n_z, shard_rows, columns = gathered.shape
    length = own.shape[0]
    wide = columns // 2
    span = n_y * shard_rows
    fetches = [
        pltpu.make_async_copy(gathered.at[y], weight.at[:, y], in_sems.at[y])
        for y in range(n_y)
    ]
    for fetch in fetches:
        fetch.start()
    first, second, third = filters[0:1, :], filters[1:2, :], filters[2:3, :]
    slope = math.sqrt(2.0 / math.pi)
    sums = [jnp.zeros((1, columns), jnp.float32) for _ in range(3)]
    for fetch in fetches:
        fetch.wait()
    stores = [pltpu.make_async_copy(weight, weight_out, out_sems.at[0])]
    stores[0].start()
    for part, rows in enumerate((own, other)):
        pre = jnp.dot(
            rows[...],
            weight[...].reshape(n_z * span, columns),
            preferred_element_type=jnp.float32,
        )
        pre = pre.astype(jnp.bfloat16).astype(jnp.float32)
        one_back, two_back = moved(pre, 1), moved(pre, 2)
        mixed = first * two_back + second * one_back + third * pre
        gate, up = mixed[:, :wide], mixed[:, wide:]
        square = gate * gate
        bend = jnp.tanh(slope * (gate + 0.044715 * (square * gate)))
        side = 0.5 * (1.0 + bend)
        active = gate * side
        rise = side + 0.5 * gate * (1.0 - bend * bend) * (
            slope * (1.0 + (3 * 0.044715) * square)
        )
        given = cotangent[part].astype(jnp.float32)
        back = jnp.concatenate([given * up * rise, given * active], axis=1)
        for tap, source in enumerate((two_back, one_back, pre)):
            sums[tap] = sums[tap] + jnp.sum(back * source, axis=0, keepdims=True)
        full = third * back + second * moved(back, -1) + first * moved(back, -2)
        grads[part * length : (part + 1) * length, :] = full.astype(jnp.bfloat16)
    stores.append(pltpu.make_async_copy(grads, grads_out, out_sems.at[1]))
    stores[1].start()
    tap_sums[...] = jnp.concatenate(
        [scale * value for value in sums]
        + [jnp.zeros((tap_sums.shape[0] - 3, columns), jnp.float32)]
    )
    for z in range(n_z):
        term = sum(
            lax.dot_general(
                rows[:, z * span : (z + 1) * span],
                grads[part * length : (part + 1) * length, :],
                contract_first,
                preferred_element_type=jnp.float32,
            )
            for part, rows in enumerate((own, other))
        )
        term = (term * scale).astype(jnp.bfloat16)
        terms[z] = term.reshape(n_y, shard_rows, columns)
        store = pltpu.make_async_copy(
            terms.at[z], terms_out.at[:, z], out_sems.at[2 + z]
        )
        store.start()
        stores.append(store)
    for store in stores:
        store.wait()


def early_pass(scale, gathered, own, other, cotangent, filters):
    n_y, n_z, shard_rows, columns = gathered.shape
    length, depth = own.shape
    whole = pl.BlockSpec(memory_space=pltpu.VMEM)
    apart = pl.BlockSpec(memory_space=pl.ANY)
    ordered = (n_z, n_y, shard_rows, columns)
    return pl.pallas_call(
        functools.partial(early_kernel, scale),
        out_shape=(
            jax.ShapeDtypeStruct(ordered, jnp.bfloat16),
            jax.ShapeDtypeStruct((2 * length, columns), jnp.bfloat16),
            jax.ShapeDtypeStruct(gathered.shape, jnp.bfloat16),
            jax.ShapeDtypeStruct((8, columns), jnp.float32),
        ),
        in_specs=[apart] + [whole] * 4,
        out_specs=(apart, apart, apart, whole),
        scratch_shapes=[
            pltpu.VMEM(ordered, jnp.bfloat16),
            pltpu.VMEM((2 * length, columns), jnp.bfloat16),
            pltpu.VMEM(ordered, jnp.bfloat16),
            pltpu.SemaphoreType.DMA((n_y,)),
            pltpu.SemaphoreType.DMA((2 + n_z,)),
        ],
        compiler_params=pltpu.CompilerParams(vmem_limit_bytes=48 * 1024 * 1024),
        cost_estimate=pl.CostEstimate(
            flops=8 * length * depth * columns,
            bytes_accessed=6 * depth * columns + 4 * length * depth,
            transcendentals=length * columns,
        ),
        name="early_pass",
    )(gathered, own, other, cotangent, filters)


def stored(product):
    return lax.optimization_barrier(product.astype(jnp.bfloat16)).astype(jnp.float32)


def per_device(
    late_rows,
    early_rows,
    hidden_cot,
    gate_weight,
    up_weight,
    gate_taps,
    up_taps,
    gate_grad_sum,
    up_grad_sum,
    gate_taps_sum,
    up_taps_sum,
):
    row_count, depth = late_rows.shape
    shard_rows, width_local = gate_weight.shape
    width = width_local // 2
    wide = -(-width // 128) * 128
    n_z = lax.axis_size("zp") * lax.axis_size("zb")
    n_y = lax.axis_size("y")
    n_x = lax.axis_size("x")
    zb = lax.axis_index("zb")
    first_z = zb == 0
    first_c = lax.axis_index("c") == 0
    rows_scale = (row_count * n_z * n_y) ** (-0.5)

    def widened(array):
        edges = [(0, 0)] * (array.ndim - 1)
        return jnp.pad(array, edges + [(0, wide - width)])

    def halves(array):
        low, high = widened(array[..., :width]), widened(array[..., width:])
        return pick(first_z, low, high), pick(first_z, high, low)

    def columns_joined(mine, other):
        return pick(
            first_z,
            jnp.concatenate([mine, other], axis=-1),
            jnp.concatenate([other, mine], axis=-1),
        )

    def partners(late, early):
        cut = row_count // 2
        sent = jnp.concatenate(
            [pick(first_c, rows[:cut], rows[cut:]) for rows in (early, late)]
        )
        here = swapped(sent, "zb")
        there = swapped(here, "c")
        low, high = pick(first_c, here, there), pick(first_c, there, here)
        return (
            jnp.concatenate([low[cut:], high[cut:]]),
            jnp.concatenate([low[:cut], high[:cut]]),
        )

    for_z = jnp.stack(
        [
            jnp.concatenate([widened(gate_weight[:, at]), widened(up_weight[:, at])], axis=1)
            for at in (slice(0, width), slice(width, 2 * width))
        ]
        * (n_z // 2)
    )
    block = lax.all_to_all(for_z, Z, 0, 0, tiled=True)
    late_other, early_other = partners(late_rows, early_rows)
    cot_mine, cot_other = halves(hidden_cot)
    cotangent = jnp.stack([cot_mine, swapped(cot_other, "zb")])
    filters = jnp.concatenate([halves(gate_taps)[0], halves(up_taps)[0]], axis=1)
    filters = jnp.pad(filters.astype(jnp.float32), [(0, 5), (0, 0)])

    block = block.reshape(n_z * shard_rows, 2 * wide)
    weight = lax.all_gather(block, "y").reshape(n_y, n_z, shard_rows, 2 * wide)
    weight, both_grads, terms, taps = early_pass(
        rows_scale, weight, early_rows, early_other, cotangent, filters
    )
    weight = weight.reshape(depth, 2 * wide)
    terms = terms.reshape(depth, 2 * wide)
    reduced = lax.psum_scatter(terms, "y", scatter_dimension=0, tiled=True)
    reduced = reduced.reshape(n_z, shard_rows, 2 * wide)
    partial = lax.dot_general(
        both_grads, weight, contract_last, preferred_element_type=jnp.float32
    ).astype(jnp.bfloat16)
    cut = depth // 2
    kept = pick(first_c, partial[:, :cut], partial[:, cut:])
    given = pick(first_c, partial[:, cut:], partial[:, :cut])
    chip = kept.astype(jnp.float32) + swapped(given, "c").astype(jnp.float32)
    chip = chip.astype(jnp.bfloat16)
    chip = chip.reshape(2, n_x, row_count // n_x, cut)
    chip = jnp.stack([pick(first_z, chip[0], chip[1]), pick(first_z, chip[1], chip[0])])
    spread = lax.all_to_all(
        chip.reshape(2 * n_x, row_count // n_x, cut), ("zb", "x"), 0, 0, tiled=True
    )
    own = jnp.sum(spread.astype(jnp.float32), axis=0).astype(jnp.bfloat16)
    copies = jnp.broadcast_to(own[None], (2 * n_x, *own.shape))
    finished = lax.all_to_all(copies, TP, 0, 0, tiled=True)
    for step in (1, 2, 4):
        taps = taps + lax.ppermute(taps, "y", [(k, k ^ step) for k in range(n_y)])
    high = lax.reduce_precision(taps, 8, 7)
    taps = jnp.concatenate([high, taps - high]).astype(jnp.bfloat16)

    product = [
        stored(jnp.dot(rows, weight, preferred_element_type=jnp.float32))
        for rows in (late_rows, late_other)
    ]
    mixed = [causal_mix(values, filters) for values in product]
    late = [
        (jax.nn.gelu(values[:, :wide], approximate=True) * values[:, wide:]).astype(
            jnp.bfloat16
        )
        for values in mixed
    ]
    late_hidden = columns_joined(late[0][:, :width], swapped(late[1], "zb")[:, :width])

    reduced, finished = lax.optimization_barrier((reduced, finished))
    reduced = jnp.concatenate(
        [reduced, jnp.broadcast_to(taps[None], (n_z, *taps.shape))], axis=1
    )
    pieces = lax.all_to_all(reduced, Z, 0, 0, tiled=True)
    pieces = pieces.reshape(2, 2, -1, 2 * wide).astype(jnp.float32)
    pieces = jnp.sum(pieces, axis=0)
    tap_sums = pieces[:, shard_rows:].reshape(2, 2, -1, 2 * wide)
    tap_sums = jnp.sum(tap_sums, axis=1)[:, :3]
    pieces = pieces[:, :shard_rows]
    gate_tap_sums = jnp.concatenate([tap_sums[0, :, :width], tap_sums[1, :, :width]], axis=1)
    up_tap_sums = jnp.concatenate(
        [tap_sums[0, :, wide : wide + width], tap_sums[1, :, wide : wide + width]], axis=1
    )
    gate_sum = jnp.concatenate([pieces[0, :, :width], pieces[1, :, :width]], axis=1)
    up_sum = jnp.concatenate([pieces[0, :, wide : wide + width], pieces[1, :, wide : wide + width]], axis=1)

    finished = finished.reshape(n_x, 2, row_count // n_x, cut)
    early_grad = finished.transpose(0, 2, 1, 3).reshape(row_count, depth)
    return (
        late_hidden,
        early_grad,
        gate_grad_sum + gate_sum,
        up_grad_sum + up_sum,
        gate_taps_sum + gate_tap_sums,
        up_taps_sum + up_tap_sums,
    )


def solution(mesh):
    split = Mesh(
        mesh.devices.reshape(mesh.shape["rep"], 2, 2, 8, 4, 2),
        ("rep", "zp", "zb", "y", "x", "c"),
    )
    placed = (
        P(REP_FS, None),
        P(REP_FS, None),
        P(REP_FS, TP),
        P(FS, TP),
        P(FS, TP),
        P(None, TP),
        P(None, TP),
        P(REP_FS, TP),
        P(REP_FS, TP),
        P("rep", TP),
        P("rep", TP),
    )
    return jax.shard_map(
        per_device,
        mesh=split,
        in_specs=placed,
        out_specs=(
            P(REP_FS, TP),
            P(REP_FS, None),
            P(REP_FS, TP),
            P(REP_FS, TP),
            P("rep", TP),
            P("rep", TP),
        ),
        check_vma=False,
    )
```

```python
import functools
import math

import jax
import jax.numpy as jnp
from jax import lax
from jax.experimental import pallas as pl
from jax.experimental.pallas import tpu as pltpu
from jax.sharding import Mesh
from jax.sharding import PartitionSpec as P

Z = ("zp", "zb")
FS = ("zp", "zb", "y")
REP_FS = ("rep", "zp", "zb", "y")
TP = ("x", "c")

contract_last = (((1,), (1,)), ((), ()))
contract_first = (((0,), (0,)), ((), ()))


def swapped(values, axis):
    return lax.ppermute(values, axis, [(0, 1), (1, 0)])


def pick(flag, first, second):
    return jnp.where(flag, first, second)


def moved(values, by):
    length = values.shape[0]
    at = lax.broadcasted_iota(jnp.int32, values.shape, 0)
    turned = pltpu.roll(values, by % length, 0)
    inside = at >= by if by > 0 else at < length + by
    return jnp.where(inside, turned, 0.0)


def early_kernel(
    scale,
    gathered,
    own,
    other,
    cotangent,
    filters_in,
    weight_out,
    grads_out,
    terms_out,
    sums_out,
    weight,
    grads,
    terms,
    filters,
    tap_sums,
    in_sems,
    out_sems,
):
    n_y, n_z, shard_rows, columns = gathered.shape
    length = own.shape[0]
    wide = columns // 2
    span = n_y * shard_rows
    fetches = [
        pltpu.make_async_copy(gathered.at[y], weight.at[:, y], in_sems.at[y])
        for y in range(n_y)
    ]
    fetches.append(pltpu.make_async_copy(filters_in, filters, in_sems.at[n_y]))
    for fetch in fetches:
        fetch.start()
    for fetch in fetches:
        fetch.wait()
    first, second, third = filters[0:1, :], filters[1:2, :], filters[2:3, :]
    slope = math.sqrt(2.0 / math.pi)
    sums = [jnp.zeros((1, columns), jnp.float32) for _ in range(3)]
    stores = [pltpu.make_async_copy(weight, weight_out, out_sems.at[0])]
    stores[0].start()
    for part, rows in enumerate((own, other)):
        pre = jnp.dot(
            rows[...],
            weight[...].reshape(n_z * span, columns),
            preferred_element_type=jnp.float32,
        )
        pre = pre.astype(jnp.bfloat16).astype(jnp.float32)
        one_back, two_back = moved(pre, 1), moved(pre, 2)
        mixed = first * two_back + second * one_back + third * pre
        gate, up = mixed[:, :wide], mixed[:, wide:]
        square = gate * gate
        bend = jnp.tanh(slope * (gate + 0.044715 * (square * gate)))
        side = 0.5 * (1.0 + bend)
        active = gate * side
        rise = side + 0.5 * gate * (1.0 - bend * bend) * (
            slope * (1.0 + (3 * 0.044715) * square)
        )
        given = cotangent[part].astype(jnp.float32)
        back = jnp.concatenate([given * up * rise, given * active], axis=1)
        for tap, source in enumerate((two_back, one_back, pre)):
            sums[tap] = sums[tap] + jnp.sum(back * source, axis=0, keepdims=True)
        full = third * back + second * moved(back, -1) + first * moved(back, -2)
        grads[part * length : (part + 1) * length, :] = full.astype(jnp.bfloat16)
    stores.append(pltpu.make_async_copy(grads, grads_out, out_sems.at[1]))
    stores[1].start()
    tap_sums[...] = jnp.concatenate(
        [scale * value for value in sums]
        + [jnp.zeros((tap_sums.shape[0] - 3, columns), jnp.float32)]
    )
    stores.append(pltpu.make_async_copy(tap_sums, sums_out, out_sems.at[2]))
    stores[2].start()
    for z in range(n_z):
        term = sum(
            lax.dot_general(
                rows[:, z * span : (z + 1) * span],
                grads[part * length : (part + 1) * length, :],
                contract_first,
                preferred_element_type=jnp.float32,
            )
            for part, rows in enumerate((own, other))
        )
        term = (term * scale).astype(jnp.bfloat16)
        terms[z] = term.reshape(n_y, shard_rows, columns)
        store = pltpu.make_async_copy(
            terms.at[z], terms_out.at[:, z], out_sems.at[3 + z]
        )
        store.start()
        stores.append(store)
    for store in stores:
        store.wait()


def early_pass(scale, gathered, own, other, cotangent, filters):
    n_y, n_z, shard_rows, columns = gathered.shape
    length, depth = own.shape
    whole = pl.BlockSpec(memory_space=pltpu.VMEM)
    apart = pl.BlockSpec(memory_space=pltpu.HBM)
    ordered = (n_z, n_y, shard_rows, columns)
    return pl.pallas_call(
        functools.partial(early_kernel, scale),
        out_shape=(
            jax.ShapeDtypeStruct(ordered, jnp.bfloat16),
            jax.ShapeDtypeStruct((2 * length, columns), jnp.bfloat16),
            jax.ShapeDtypeStruct(gathered.shape, jnp.bfloat16),
            jax.ShapeDtypeStruct((8, columns), jnp.float32),
        ),
        in_specs=[apart] + [whole] * 3 + [apart],
        out_specs=(apart,) * 4,
        scratch_shapes=[
            pltpu.VMEM(ordered, jnp.bfloat16),
            pltpu.VMEM((2 * length, columns), jnp.bfloat16),
            pltpu.VMEM(ordered, jnp.bfloat16),
            pltpu.VMEM((8, columns), jnp.float32),
            pltpu.VMEM((8, columns), jnp.float32),
            pltpu.SemaphoreType.DMA((n_y + 1,)),
            pltpu.SemaphoreType.DMA((3 + n_z,)),
        ],
        compiler_params=pltpu.CompilerParams(vmem_limit_bytes=57 * 1024 * 1024),
        cost_estimate=pl.CostEstimate(
            flops=8 * length * depth * columns,
            bytes_accessed=6 * depth * columns + 4 * length * depth,
            transcendentals=length * columns,
        ),
        name="early_pass",
    )(gathered, own, other, cotangent, filters)


def late_kernel(weight_in, own, other, filters_in, hidden, weight, filters, in_sems):
    wide = hidden.shape[2]
    fetches = [
        pltpu.make_async_copy(weight_in, weight, in_sems.at[0]),
        pltpu.make_async_copy(filters_in, filters, in_sems.at[1]),
    ]
    for fetch in fetches:
        fetch.start()
    for fetch in fetches:
        fetch.wait()
    first, second, third = filters[0:1, :], filters[1:2, :], filters[2:3, :]
    slope = math.sqrt(2.0 / math.pi)
    for part, rows in enumerate((own, other)):
        pre = jnp.dot(rows[...], weight[...], preferred_element_type=jnp.float32)
        pre = pre.astype(jnp.bfloat16).astype(jnp.float32)
        mixed = first * moved(pre, 2) + second * moved(pre, 1) + third * pre
        gate, up = mixed[:, :wide], mixed[:, wide:]
        bend = jnp.tanh(slope * (gate + 0.044715 * (gate * gate * gate)))
        hidden[part] = (0.5 * gate * (1.0 + bend) * up).astype(jnp.bfloat16)


def late_pass(weight, own, other, filters):
    depth, columns = weight.shape
    length = own.shape[0]
    whole = pl.BlockSpec(memory_space=pltpu.VMEM)
    apart = pl.BlockSpec(memory_space=pltpu.HBM)
    return pl.pallas_call(
        late_kernel,
        out_shape=jax.ShapeDtypeStruct((2, length, columns // 2), jnp.bfloat16),
        in_specs=[apart, whole, whole, apart],
        out_specs=whole,
        scratch_shapes=[
            pltpu.VMEM(weight.shape, jnp.bfloat16),
            pltpu.VMEM(filters.shape, jnp.float32),
            pltpu.SemaphoreType.DMA((2,)),
        ],
        compiler_params=pltpu.CompilerParams(vmem_limit_bytes=58 * 1024 * 1024),
        cost_estimate=pl.CostEstimate(
            flops=4 * length * depth * columns,
            bytes_accessed=2 * depth * columns + 4 * length * depth,
            transcendentals=length * columns,
        ),
        name="late_pass",
    )(weight, own, other, filters)


def per_device(
    late_rows,
    early_rows,
    hidden_cot,
    gate_weight,
    up_weight,
    gate_taps,
    up_taps,
    gate_grad_sum,
    up_grad_sum,
    gate_taps_sum,
    up_taps_sum,
):
    row_count, depth = late_rows.shape
    shard_rows, width_local = gate_weight.shape
    wide = -(-width_local // 256) * 128
    rest = width_local - wide
    n_z = lax.axis_size("zp") * lax.axis_size("zb")
    n_y = lax.axis_size("y")
    n_x = lax.axis_size("x")
    zb = lax.axis_index("zb")
    first_z = zb == 0
    first_c = lax.axis_index("c") == 0
    rows_scale = (row_count * n_z * n_y) ** (-0.5)

    def low_high(array):
        edges = [(0, 0)] * (array.ndim - 1)
        return array[..., :wide], jnp.pad(array[..., wide:], edges + [(0, wide - rest)])

    def halves(array):
        low, high = low_high(array)
        return pick(first_z, low, high), pick(first_z, high, low)

    def joined(low, high):
        return jnp.concatenate([low, high[..., :rest]], axis=-1)

    def partners(late, early):
        cut = row_count // 2
        sent = jnp.concatenate(
            [pick(first_c, rows[:cut], rows[cut:]) for rows in (early, late)]
        )
        here = swapped(sent, "zb")
        there = swapped(here, "c")
        low, high = pick(first_c, here, there), pick(first_c, there, here)
        return (
            jnp.concatenate([low[cut:], high[cut:]]),
            jnp.concatenate([low[:cut], high[:cut]]),
        )

    sides = [
        jnp.concatenate(pair, axis=1)
        for pair in zip(low_high(gate_weight), low_high(up_weight))
    ]
    for_z = jnp.stack(sides * (n_z // 2))
    block = lax.all_to_all(for_z, Z, 0, 0, tiled=True)
    late_other, early_other = partners(late_rows, early_rows)
    cot_mine, cot_other = halves(hidden_cot)
    cotangent = jnp.stack([cot_mine, swapped(cot_other, "zb")])
    filters = jnp.concatenate([halves(gate_taps)[0], halves(up_taps)[0]], axis=1)
    filters = jnp.pad(filters.astype(jnp.float32), [(0, 5), (0, 0)])

    block = block.reshape(n_z * shard_rows, 2 * wide)
    weight = lax.all_gather(block, "y").reshape(n_y, n_z, shard_rows, 2 * wide)
    weight, both_grads, terms, taps = early_pass(
        rows_scale, weight, early_rows, early_other, cotangent, filters
    )
    weight = weight.reshape(depth, 2 * wide)
    terms = terms.reshape(depth, 2 * wide)
    reduced = lax.psum_scatter(terms, "y", scatter_dimension=0, tiled=True)
    reduced = reduced.reshape(n_z, shard_rows, 2 * wide)
    partial = lax.dot_general(
        both_grads, weight, contract_last, preferred_element_type=jnp.float32
    ).astype(jnp.bfloat16)
    cut = depth // 2
    kept = pick(first_c, partial[:, :cut], partial[:, cut:])
    given = pick(first_c, partial[:, cut:], partial[:, :cut])
    chip = kept.astype(jnp.float32) + swapped(given, "c").astype(jnp.float32)
    chip = chip.astype(jnp.bfloat16)
    chip = chip.reshape(2, n_x, row_count // n_x, cut)
    chip = jnp.stack([pick(first_z, chip[0], chip[1]), pick(first_z, chip[1], chip[0])])
    spread = lax.all_to_all(
        chip.reshape(2 * n_x, row_count // n_x, cut), ("zb", "x"), 0, 0, tiled=True
    )
    own = jnp.sum(spread.astype(jnp.float32), axis=0).astype(jnp.bfloat16)
    copies = jnp.broadcast_to(own[None], (n_x, *own.shape))
    finished = lax.all_to_all(copies, "x", 0, 0, tiled=True).reshape(row_count, cut)
    for step in (1, 2, 4):
        taps = taps + lax.ppermute(taps, "y", [(k, k ^ step) for k in range(n_y)])
    high = lax.reduce_precision(taps, 8, 7)
    taps = jnp.concatenate([high, taps - high]).astype(jnp.bfloat16)

    late = late_pass(weight, late_rows, late_other, filters)
    late_there = swapped(late[1], "zb")

    start = jnp.broadcast_to(taps[None], (n_z, *taps.shape))
    start = jnp.pad(start, [(0, 0), (shard_rows, 0), (0, 0)])
    reduced, finished, late_there, start = lax.optimization_barrier(
        (reduced, finished, late_there, start)
    )
    reduced = lax.dynamic_update_slice(start, reduced, (0, 0, 0))
    pieces = lax.all_to_all(reduced, Z, 0, 0, tiled=True)
    pieces = pieces.reshape(2, 2, -1, 2 * wide).astype(jnp.float32)
    pieces = jnp.sum(pieces, axis=0)
    tap_sums = pieces[:, shard_rows:].reshape(2, 2, -1, 2 * wide)
    tap_sums = jnp.sum(tap_sums, axis=1)[:, :3]
    pieces = pieces[:, :shard_rows]
    beside = swapped(finished, "c")
    early_grad = pick(
        first_c,
        jnp.concatenate([finished, beside], axis=1),
        jnp.concatenate([beside, finished], axis=1),
    )
    late_hidden = joined(
        pick(first_z, late[0], late_there), pick(first_z, late_there, late[0])
    )
    return (
        late_hidden,
        early_grad,
        gate_grad_sum + joined(pieces[0, :, :wide], pieces[1, :, :wide]),
        up_grad_sum + joined(pieces[0, :, wide:], pieces[1, :, wide:]),
        gate_taps_sum + joined(tap_sums[0, :, :wide], tap_sums[1, :, :wide]),
        up_taps_sum + joined(tap_sums[0, :, wide:], tap_sums[1, :, wide:]),
    )


def solution(mesh):
    split = Mesh(
        mesh.devices.reshape(mesh.shape["rep"], 2, 2, 8, 4, 2),
        ("rep", "zp", "zb", "y", "x", "c"),
    )
    placed = (
        P(REP_FS, None),
        P(REP_FS, None),
        P(REP_FS, TP),
        P(FS, TP),
        P(FS, TP),
        P(None, TP),
        P(None, TP),
        P(REP_FS, TP),
        P(REP_FS, TP),
        P("rep", TP),
        P("rep", TP),
    )
    return jax.shard_map(
        per_device,
        mesh=split,
        in_specs=placed,
        out_specs=(
            P(REP_FS, TP),
            P(REP_FS, None),
            P(REP_FS, TP),
            P(REP_FS, TP),
            P("rep", TP),
            P("rep", TP),
        ),
        check_vma=False,
    )
```

```python
import functools
import math

import jax
import jax.numpy as jnp
from jax import lax
from jax.experimental import pallas as pl
from jax.experimental.pallas import tpu as pltpu
from jax.sharding import Mesh
from jax.sharding import PartitionSpec as P

Z = ("zp", "zb")
FS = ("zp", "zb", "y")
REP_FS = ("rep", "zp", "zb", "y")
TP = ("x", "c")

contract_last = (((1,), (1,)), ((), ()))
contract_first = (((0,), (0,)), ((), ()))


def swapped(values, axis):
    return lax.ppermute(values, axis, [(0, 1), (1, 0)])


def pick(flag, first, second):
    return jnp.where(flag, first, second)


def moved(values, by):
    length = values.shape[0]
    at = lax.broadcasted_iota(jnp.int32, values.shape, 0)
    turned = pltpu.roll(values, by % length, 0)
    inside = at >= by if by > 0 else at < length + by
    return jnp.where(inside, turned, 0.0)


def early_kernel(
    scale,
    gathered,
    own_in,
    low_in,
    high_in,
    cotangent_in,
    filters_in,
    weight_out,
    grads_out,
    terms_out,
    sums_out,
    weight,
    grads,
    terms,
    own,
    other,
    cotangent,
    filters,
    tap_sums,
    in_sems,
    out_sems,
):
    n_y, n_z, shard_rows, columns = gathered.shape
    length = own.shape[0]
    cut = length // 2
    wide = columns // 2
    span = n_y * shard_rows
    fetches = [
        pltpu.make_async_copy(gathered.at[y], weight.at[:, y], in_sems.at[y])
        for y in range(n_y)
    ]
    pairs = (
        (own_in, own),
        (filters_in, filters),
        (cotangent_in, cotangent),
        (low_in.at[:cut], other.at[:cut]),
        (high_in.at[:cut], other.at[cut:]),
    )
    fetches += [
        pltpu.make_async_copy(source, target, in_sems.at[n_y + at])
        for at, (source, target) in enumerate(pairs)
    ]
    for fetch in fetches:
        fetch.start()
    for fetch in fetches:
        fetch.wait()
    first, second, third = filters[0:1, :], filters[1:2, :], filters[2:3, :]
    slope = math.sqrt(2.0 / math.pi)
    sums = [jnp.zeros((1, columns), jnp.float32) for _ in range(3)]
    stores = [pltpu.make_async_copy(weight, weight_out, out_sems.at[0])]
    stores[0].start()
    for part, rows in enumerate((own, other)):
        pre = jnp.dot(
            rows[...],
            weight[...].reshape(n_z * span, columns),
            preferred_element_type=jnp.float32,
        )
        pre = pre.astype(jnp.bfloat16).astype(jnp.float32)
        one_back, two_back = moved(pre, 1), moved(pre, 2)
        mixed = first * two_back + second * one_back + third * pre
        gate, up = mixed[:, :wide], mixed[:, wide:]
        square = gate * gate
        bend = jnp.tanh(slope * (gate + 0.044715 * (square * gate)))
        side = 0.5 * (1.0 + bend)
        active = gate * side
        rise = side + 0.5 * gate * (1.0 - bend * bend) * (
            slope * (1.0 + (3 * 0.044715) * square)
        )
        given = cotangent[part].astype(jnp.float32)
        back = jnp.concatenate([given * up * rise, given * active], axis=1)
        for tap, source in enumerate((two_back, one_back, pre)):
            sums[tap] = sums[tap] + jnp.sum(back * source, axis=0, keepdims=True)
        full = third * back + second * moved(back, -1) + first * moved(back, -2)
        grads[part * length : (part + 1) * length, :] = full.astype(jnp.bfloat16)
    stores.append(pltpu.make_async_copy(grads, grads_out, out_sems.at[1]))
    stores[1].start()
    tap_sums[...] = jnp.concatenate(
        [scale * value for value in sums]
        + [jnp.zeros((tap_sums.shape[0] - 3, columns), jnp.float32)]
    )
    stores.append(pltpu.make_async_copy(tap_sums, sums_out, out_sems.at[2]))
    stores[2].start()
    for z in range(n_z):
        term = sum(
            lax.dot_general(
                rows[:, z * span : (z + 1) * span],
                grads[part * length : (part + 1) * length, :],
                contract_first,
                preferred_element_type=jnp.float32,
            )
            for part, rows in enumerate((own, other))
        )
        term = (term * scale).astype(jnp.bfloat16)
        terms[z] = term.reshape(n_y, shard_rows, columns)
        store = pltpu.make_async_copy(
            terms.at[z], terms_out.at[:, z], out_sems.at[3 + z]
        )
        store.start()
        stores.append(store)
    for store in stores:
        store.wait()


def early_pass(scale, gathered, own, low, high, cotangent, filters):
    n_y, n_z, shard_rows, columns = gathered.shape
    length, depth = own.shape
    apart = pl.BlockSpec(memory_space=pltpu.HBM)
    ordered = (n_z, n_y, shard_rows, columns)
    return pl.pallas_call(
        functools.partial(early_kernel, scale),
        out_shape=(
            jax.ShapeDtypeStruct(ordered, jnp.bfloat16),
            jax.ShapeDtypeStruct((2 * length, columns), jnp.bfloat16),
            jax.ShapeDtypeStruct(gathered.shape, jnp.bfloat16),
            jax.ShapeDtypeStruct((8, columns), jnp.float32),
        ),
        in_specs=[apart] * 6,
        out_specs=(apart,) * 4,
        scratch_shapes=[
            pltpu.VMEM(ordered, jnp.bfloat16),
            pltpu.VMEM((2 * length, columns), jnp.bfloat16),
            pltpu.VMEM(ordered, jnp.bfloat16),
            pltpu.VMEM(own.shape, jnp.bfloat16),
            pltpu.VMEM(own.shape, jnp.bfloat16),
            pltpu.VMEM(cotangent.shape, jnp.bfloat16),
            pltpu.VMEM((8, columns), jnp.float32),
            pltpu.VMEM((8, columns), jnp.float32),
            pltpu.SemaphoreType.DMA((n_y + 5,)),
            pltpu.SemaphoreType.DMA((3 + n_z,)),
        ],
        compiler_params=pltpu.CompilerParams(vmem_limit_bytes=57 * 1024 * 1024),
        cost_estimate=pl.CostEstimate(
            flops=8 * length * depth * columns,
            bytes_accessed=6 * depth * columns + 4 * length * depth,
            transcendentals=length * columns,
        ),
        name="early_pass",
    )(gathered, own, low, high, cotangent, filters)


def late_kernel(
    weight_in,
    own_in,
    low_in,
    high_in,
    filters_in,
    mine,
    theirs,
    weight,
    own,
    other,
    filters,
    in_sems,
):
    length, wide = mine.shape
    cut = length // 2
    pairs = (
        (own_in, own),
        (weight_in, weight),
        (filters_in, filters),
        (low_in.at[cut:], other.at[:cut]),
        (high_in.at[cut:], other.at[cut:]),
    )
    fetches = [
        pltpu.make_async_copy(source, target, in_sems.at[at])
        for at, (source, target) in enumerate(pairs)
    ]
    for fetch in fetches:
        fetch.start()
    for fetch in fetches:
        fetch.wait()
    first, second, third = filters[0:1, :], filters[1:2, :], filters[2:3, :]
    slope = math.sqrt(2.0 / math.pi)
    for rows, hidden in ((other, theirs), (own, mine)):
        pre = jnp.dot(rows[...], weight[...], preferred_element_type=jnp.float32)
        pre = pre.astype(jnp.bfloat16).astype(jnp.float32)
        mixed = first * moved(pre, 2) + second * moved(pre, 1) + third * pre
        gate, up = mixed[:, :wide], mixed[:, wide:]
        bend = jnp.tanh(slope * (gate + 0.044715 * (gate * gate * gate)))
        hidden[...] = (0.5 * gate * (1.0 + bend) * up).astype(jnp.bfloat16)


def late_pass(weight, own, low, high, filters):
    depth, columns = weight.shape
    length = own.shape[0]
    whole = pl.BlockSpec(memory_space=pltpu.VMEM)
    apart = pl.BlockSpec(memory_space=pltpu.HBM)
    part = jax.ShapeDtypeStruct((length, columns // 2), jnp.bfloat16)
    return pl.pallas_call(
        late_kernel,
        out_shape=(part, part),
        in_specs=[apart] * 5,
        out_specs=(whole, whole),
        scratch_shapes=[
            pltpu.VMEM(weight.shape, jnp.bfloat16),
            pltpu.VMEM(own.shape, jnp.bfloat16),
            pltpu.VMEM(own.shape, jnp.bfloat16),
            pltpu.VMEM(filters.shape, jnp.float32),
            pltpu.SemaphoreType.DMA((5,)),
        ],
        compiler_params=pltpu.CompilerParams(vmem_limit_bytes=58 * 1024 * 1024),
        cost_estimate=pl.CostEstimate(
            flops=4 * length * depth * columns,
            bytes_accessed=2 * depth * columns + 4 * length * depth,
            transcendentals=length * columns,
        ),
        name="late_pass",
    )(weight, own, low, high, filters)


def pack_kernel(gate, up, packed):
    wide = packed.shape[2] // 2
    rows, width = gate.shape
    blank = jnp.zeros((rows, 2 * wide - width), packed.dtype)
    for at, source in ((0, gate), (wide, up)):
        low = source[:, :wide]
        high = jnp.concatenate([source[:, wide:], blank], axis=1)
        for z in range(packed.shape[0]):
            packed[z, :, at : at + wide] = high if z % 2 else low


def packed_halves(gate, up, wide, count):
    whole = pl.BlockSpec(memory_space=pltpu.VMEM)
    return pl.pallas_call(
        pack_kernel,
        out_shape=jax.ShapeDtypeStruct((count, gate.shape[0], 2 * wide), gate.dtype),
        in_specs=[whole] * 2,
        out_specs=whole,
        name="pack_halves",
    )(gate, up)


def per_device(
    late_rows,
    early_rows,
    hidden_cot,
    gate_weight,
    up_weight,
    gate_taps,
    up_taps,
    gate_grad_sum,
    up_grad_sum,
    gate_taps_sum,
    up_taps_sum,
):
    row_count, depth = late_rows.shape
    shard_rows, width_local = gate_weight.shape
    wide = -(-width_local // 256) * 128
    rest = width_local - wide
    n_z = lax.axis_size("zp") * lax.axis_size("zb")
    n_y = lax.axis_size("y")
    n_x = lax.axis_size("x")
    zb = lax.axis_index("zb")
    first_z = zb == 0
    first_c = lax.axis_index("c") == 0
    rows_scale = (row_count * n_z * n_y) ** (-0.5)

    def low_high(array):
        edges = [(0, 0)] * (array.ndim - 1)
        return array[..., :wide], jnp.pad(array[..., wide:], edges + [(0, wide - rest)])

    def halves(array):
        low, high = low_high(array)
        return pick(first_z, low, high), pick(first_z, high, low)

    def joined(low, high):
        return jnp.concatenate([low, high[..., :rest]], axis=-1)

    for_z = packed_halves(gate_weight, up_weight, wide, n_z)
    block = lax.all_to_all(for_z, Z, 0, 0, tiled=True)
    half = row_count // 2
    sent = jnp.concatenate(
        [pick(first_c, rows[:half], rows[half:]) for rows in (early_rows, late_rows)]
    )
    here = swapped(sent, "zb")
    there = swapped(here, "c")
    low, high = pick(first_c, here, there), pick(first_c, there, here)
    cot_mine, cot_other = halves(hidden_cot)
    cotangent = jnp.stack([cot_mine, swapped(cot_other, "zb")])
    filters = jnp.concatenate([halves(gate_taps)[0], halves(up_taps)[0]], axis=1)
    filters = jnp.pad(filters.astype(jnp.float32), [(0, 5), (0, 0)])

    block = block.reshape(n_z * shard_rows, 2 * wide)
    weight = lax.all_gather(block, "y").reshape(n_y, n_z, shard_rows, 2 * wide)
    weight, both_grads, terms, taps = early_pass(
        rows_scale, weight, early_rows, low, high, cotangent, filters
    )
    weight = weight.reshape(depth, 2 * wide)
    terms = terms.reshape(depth, 2 * wide)
    reduced = lax.psum_scatter(terms, "y", scatter_dimension=0, tiled=True)
    reduced = reduced.reshape(n_z, shard_rows, 2 * wide)
    def taps_over(values, step):
        return values + lax.ppermute(values, "y", [(k, k ^ step) for k in range(n_y)])

    partial = lax.dot_general(
        both_grads, weight, contract_last, preferred_element_type=jnp.float32
    ).astype(jnp.bfloat16)
    cut = depth // 2
    kept = pick(first_c, partial[:, :cut], partial[:, cut:])
    given = pick(first_c, partial[:, cut:], partial[:, :cut])
    taken, taps = lax.optimization_barrier((swapped(given, "c"), taps_over(taps, 1)))
    chip = kept.astype(jnp.float32) + taken.astype(jnp.float32)
    chip = chip.astype(jnp.bfloat16)
    chip = chip.reshape(2, n_x, row_count // n_x, cut)
    chip = jnp.stack([pick(first_z, chip[0], chip[1]), pick(first_z, chip[1], chip[0])])
    spread = lax.all_to_all(
        chip.reshape(2 * n_x, row_count // n_x, cut), ("zb", "x"), 0, 0, tiled=True
    )
    late_here, late_sent = late_pass(weight, late_rows, low, high, filters)
    taps = taps_over(taps_over(taps, 2), 4)
    spread, late_here, late_sent, taps = lax.optimization_barrier(
        (spread, late_here, late_sent, taps)
    )
    own = jnp.sum(spread.astype(jnp.float32), axis=0).astype(jnp.bfloat16)
    copies = jnp.broadcast_to(own[None], (n_x, *own.shape))
    finished = lax.all_to_all(copies, "x", 0, 0, tiled=True).reshape(row_count, cut)
    taps = taps + swapped(taps, "zp")
    taps_there = swapped(taps, "zb")

    late_there = swapped(late_sent, "zb")

    reduced, finished, late_there, taps_there = lax.optimization_barrier(
        (reduced, finished, late_there, taps_there)
    )
    pieces = lax.all_to_all(reduced, Z, 0, 0, tiled=True)
    pieces = pieces.reshape(2, 2, shard_rows, 2 * wide).astype(jnp.float32)
    pieces = jnp.sum(pieces, axis=0)

    def both(mine, other):
        return joined(pick(first_z, mine, other), pick(first_z, other, mine))

    beside = swapped(finished, "c")
    early_grad = pick(
        first_c,
        jnp.concatenate([finished, beside], axis=1),
        jnp.concatenate([beside, finished], axis=1),
    )
    late_hidden = both(late_here, late_there)
    return (
        late_hidden,
        early_grad,
        gate_grad_sum + joined(pieces[0, :, :wide], pieces[1, :, :wide]),
        up_grad_sum + joined(pieces[0, :, wide:], pieces[1, :, wide:]),
        gate_taps_sum + both(taps[:3, :wide], taps_there[:3, :wide]),
        up_taps_sum + both(taps[:3, wide:], taps_there[:3, wide:]),
    )


def solution(mesh):
    split = Mesh(
        mesh.devices.reshape(mesh.shape["rep"], 2, 2, 8, 4, 2),
        ("rep", "zp", "zb", "y", "x", "c"),
    )
    placed = (
        P(REP_FS, None),
        P(REP_FS, None),
        P(REP_FS, TP),
        P(FS, TP),
        P(FS, TP),
        P(None, TP),
        P(None, TP),
        P(REP_FS, TP),
        P(REP_FS, TP),
        P("rep", TP),
        P("rep", TP),
    )
    return jax.shard_map(
        per_device,
        mesh=split,
        in_specs=placed,
        out_specs=(
            P(REP_FS, TP),
            P(REP_FS, None),
            P(REP_FS, TP),
            P(REP_FS, TP),
            P("rep", TP),
            P("rep", TP),
        ),
        check_vma=False,
    )
```

```python
import functools
import math

import jax
import jax.numpy as jnp
from jax import lax
from jax.experimental import pallas as pl
from jax.experimental.pallas import tpu as pltpu
from jax.sharding import Mesh
from jax.sharding import PartitionSpec as P

Z = ("zp", "zb")
FS = ("zp", "zb", "y")
REP_FS = ("rep", "zp", "zb", "y")
TP = ("x", "c")
EXTRA = 8

contract_last = (((1,), (1,)), ((), ()))
contract_first = (((0,), (0,)), ((), ()))


def swapped(values, axis):
    return lax.ppermute(values, axis, [(0, 1), (1, 0)])


def pick(flag, first, second):
    return jnp.where(flag, first, second)


def moved(values, by):
    length = values.shape[0]
    at = lax.broadcasted_iota(jnp.int32, values.shape, 0)
    turned = pltpu.roll(values, by % length, 0)
    inside = at >= by if by > 0 else at < length + by
    return jnp.where(inside, turned, 0.0)


def early_kernel(
    scale,
    gathered,
    own_in,
    low_in,
    high_in,
    cotangent_in,
    filters_in,
    weight_out,
    grads_out,
    terms_out,
    weight,
    grads,
    terms,
    own,
    other,
    cotangent,
    filters,
    in_sems,
    out_sems,
):
    n_y, n_z, shard_rows, columns = gathered.shape
    length = own.shape[0]
    cut = length // 2
    wide = columns // 2
    span = n_y * shard_rows
    fetches = [
        pltpu.make_async_copy(gathered.at[y], weight.at[:, y], in_sems.at[y])
        for y in range(n_y)
    ]
    pairs = (
        (own_in, own),
        (filters_in, filters),
        (cotangent_in, cotangent),
        (low_in.at[:cut], other.at[:cut]),
        (high_in.at[:cut], other.at[cut:]),
    )
    fetches += [
        pltpu.make_async_copy(source, target, in_sems.at[n_y + at])
        for at, (source, target) in enumerate(pairs)
    ]
    for fetch in fetches:
        fetch.start()
    for fetch in fetches:
        fetch.wait()
    first, second, third = filters[0:1, :], filters[1:2, :], filters[2:3, :]
    slope = math.sqrt(2.0 / math.pi)
    sums = [jnp.zeros((1, columns), jnp.float32) for _ in range(3)]
    stores = [pltpu.make_async_copy(weight, weight_out, out_sems.at[0])]
    stores[0].start()
    for part, rows in enumerate((own, other)):
        pre = jnp.dot(
            rows[...],
            weight[...].reshape(n_z * span, columns),
            preferred_element_type=jnp.float32,
        )
        pre = pre.astype(jnp.bfloat16).astype(jnp.float32)
        one_back, two_back = moved(pre, 1), moved(pre, 2)
        mixed = first * two_back + second * one_back + third * pre
        gate, up = mixed[:, :wide], mixed[:, wide:]
        square = gate * gate
        bend = jnp.tanh(slope * (gate + 0.044715 * (square * gate)))
        side = 0.5 * (1.0 + bend)
        active = gate * side
        rise = side + 0.5 * gate * (1.0 - bend * bend) * (
            slope * (1.0 + (3 * 0.044715) * square)
        )
        given = cotangent[part].astype(jnp.float32)
        back = jnp.concatenate([given * up * rise, given * active], axis=1)
        for tap, source in enumerate((two_back, one_back, pre)):
            sums[tap] = sums[tap] + jnp.sum(back * source, axis=0, keepdims=True)
        full = third * back + second * moved(back, -1) + first * moved(back, -2)
        grads[part * length : (part + 1) * length, :] = full.astype(jnp.bfloat16)
    stores.append(pltpu.make_async_copy(grads, grads_out, out_sems.at[1]))
    stores[1].start()
    taps = [scale * value for value in sums]
    high = [value.astype(jnp.bfloat16).astype(jnp.float32) for value in taps]
    blank = jnp.zeros((terms.shape[2] - shard_rows - 6, columns), jnp.float32)
    extra = high + [value - top for value, top in zip(taps, high)] + [blank]
    extra = jnp.concatenate(extra).astype(jnp.bfloat16)
    for z in range(n_z):
        term = sum(
            lax.dot_general(
                rows[:, z * span : (z + 1) * span],
                grads[part * length : (part + 1) * length, :],
                contract_first,
                preferred_element_type=jnp.float32,
            )
            for part, rows in enumerate((own, other))
        )
        term = (term * scale).astype(jnp.bfloat16)
        for y in range(n_y):
            terms[z, y, :shard_rows] = term[y * shard_rows : (y + 1) * shard_rows]
            terms[z, y, shard_rows:] = extra
        store = pltpu.make_async_copy(
            terms.at[z], terms_out.at[:, z], out_sems.at[2 + z]
        )
        store.start()
        stores.append(store)
    for store in stores:
        store.wait()


def early_pass(scale, gathered, own, low, high, cotangent, filters):
    n_y, n_z, shard_rows, columns = gathered.shape
    length, depth = own.shape
    apart = pl.BlockSpec(memory_space=pltpu.HBM)
    ordered = (n_z, n_y, shard_rows, columns)
    return pl.pallas_call(
        functools.partial(early_kernel, scale),
        out_shape=(
            jax.ShapeDtypeStruct(ordered, jnp.bfloat16),
            jax.ShapeDtypeStruct((2 * length, columns), jnp.bfloat16),
            jax.ShapeDtypeStruct((n_y, n_z, shard_rows + EXTRA, columns), jnp.bfloat16),
        ),
        in_specs=[apart] * 6,
        out_specs=(apart,) * 3,
        scratch_shapes=[
            pltpu.VMEM(ordered, jnp.bfloat16),
            pltpu.VMEM((2 * length, columns), jnp.bfloat16),
            pltpu.VMEM((n_z, n_y, shard_rows + EXTRA, columns), jnp.bfloat16),
            pltpu.VMEM(own.shape, jnp.bfloat16),
            pltpu.VMEM(own.shape, jnp.bfloat16),
            pltpu.VMEM(cotangent.shape, jnp.bfloat16),
            pltpu.VMEM((8, columns), jnp.float32),
            pltpu.SemaphoreType.DMA((n_y + 5,)),
            pltpu.SemaphoreType.DMA((2 + n_z,)),
        ],
        compiler_params=pltpu.CompilerParams(vmem_limit_bytes=57 * 1024 * 1024),
        cost_estimate=pl.CostEstimate(
            flops=8 * length * depth * columns,
            bytes_accessed=6 * depth * columns + 4 * length * depth,
            transcendentals=length * columns,
        ),
        name="early_pass",
    )(gathered, own, low, high, cotangent, filters)


def late_kernel(
    weight_in,
    own_in,
    low_in,
    high_in,
    filters_in,
    mine,
    theirs,
    weight,
    own,
    other,
    filters,
    in_sems,
):
    length, wide = mine.shape
    cut = length // 2
    pairs = (
        (own_in, own),
        (weight_in, weight),
        (filters_in, filters),
        (low_in.at[cut:], other.at[:cut]),
        (high_in.at[cut:], other.at[cut:]),
    )
    fetches = [
        pltpu.make_async_copy(source, target, in_sems.at[at])
        for at, (source, target) in enumerate(pairs)
    ]
    for fetch in fetches:
        fetch.start()
    for fetch in fetches:
        fetch.wait()
    first, second, third = filters[0:1, :], filters[1:2, :], filters[2:3, :]
    slope = math.sqrt(2.0 / math.pi)
    for rows, hidden in ((other, theirs), (own, mine)):
        pre = jnp.dot(rows[...], weight[...], preferred_element_type=jnp.float32)
        pre = pre.astype(jnp.bfloat16).astype(jnp.float32)
        mixed = first * moved(pre, 2) + second * moved(pre, 1) + third * pre
        gate, up = mixed[:, :wide], mixed[:, wide:]
        bend = jnp.tanh(slope * (gate + 0.044715 * (gate * gate * gate)))
        hidden[...] = (0.5 * gate * (1.0 + bend) * up).astype(jnp.bfloat16)


def late_pass(weight, own, low, high, filters):
    depth, columns = weight.shape
    length = own.shape[0]
    whole = pl.BlockSpec(memory_space=pltpu.VMEM)
    apart = pl.BlockSpec(memory_space=pltpu.HBM)
    part = jax.ShapeDtypeStruct((length, columns // 2), jnp.bfloat16)
    return pl.pallas_call(
        late_kernel,
        out_shape=(part, part),
        in_specs=[apart] * 5,
        out_specs=(whole, whole),
        scratch_shapes=[
            pltpu.VMEM(weight.shape, jnp.bfloat16),
            pltpu.VMEM(own.shape, jnp.bfloat16),
            pltpu.VMEM(own.shape, jnp.bfloat16),
            pltpu.VMEM(filters.shape, jnp.float32),
            pltpu.SemaphoreType.DMA((5,)),
        ],
        compiler_params=pltpu.CompilerParams(vmem_limit_bytes=58 * 1024 * 1024),
        cost_estimate=pl.CostEstimate(
            flops=4 * length * depth * columns,
            bytes_accessed=2 * depth * columns + 4 * length * depth,
            transcendentals=length * columns,
        ),
        name="late_pass",
    )(weight, own, low, high, filters)


def pack_kernel(gate, up, packed):
    wide = packed.shape[2] // 2
    rows, width = gate.shape
    blank = jnp.zeros((rows, 2 * wide - width), packed.dtype)
    for at, source in ((0, gate), (wide, up)):
        low = source[:, :wide]
        high = jnp.concatenate([source[:, wide:], blank], axis=1)
        for z in range(packed.shape[0]):
            packed[z, :, at : at + wide] = high if z % 2 else low


def packed_halves(gate, up, wide, count):
    whole = pl.BlockSpec(memory_space=pltpu.VMEM)
    return pl.pallas_call(
        pack_kernel,
        out_shape=jax.ShapeDtypeStruct((count, gate.shape[0], 2 * wide), gate.dtype),
        in_specs=[whole] * 2,
        out_specs=whole,
        name="pack_halves",
    )(gate, up)


def per_device(
    late_rows,
    early_rows,
    hidden_cot,
    gate_weight,
    up_weight,
    gate_taps,
    up_taps,
    gate_grad_sum,
    up_grad_sum,
    gate_taps_sum,
    up_taps_sum,
):
    row_count, depth = late_rows.shape
    shard_rows, width_local = gate_weight.shape
    wide = -(-width_local // 256) * 128
    rest = width_local - wide
    n_z = lax.axis_size("zp") * lax.axis_size("zb")
    n_y = lax.axis_size("y")
    n_x = lax.axis_size("x")
    zb = lax.axis_index("zb")
    first_z = zb == 0
    first_c = lax.axis_index("c") == 0
    rows_scale = (row_count * n_z * n_y) ** (-0.5)

    def low_high(array):
        edges = [(0, 0)] * (array.ndim - 1)
        return array[..., :wide], jnp.pad(array[..., wide:], edges + [(0, wide - rest)])

    def halves(array):
        low, high = low_high(array)
        return pick(first_z, low, high), pick(first_z, high, low)

    def joined(low, high):
        return jnp.concatenate([low, high[..., :rest]], axis=-1)

    for_z = packed_halves(gate_weight, up_weight, wide, n_z)
    block = lax.all_to_all(for_z, Z, 0, 0, tiled=True)
    half = row_count // 2
    sent = jnp.concatenate(
        [pick(first_c, rows[:half], rows[half:]) for rows in (early_rows, late_rows)]
    )
    here = swapped(sent, "zb")
    there = swapped(here, "c")
    low, high = pick(first_c, here, there), pick(first_c, there, here)
    cot_mine, cot_other = halves(hidden_cot)
    cotangent = jnp.stack([cot_mine, swapped(cot_other, "zb")])
    filters = jnp.concatenate([halves(gate_taps)[0], halves(up_taps)[0]], axis=1)
    filters = jnp.pad(filters.astype(jnp.float32), [(0, 5), (0, 0)])

    block = block.reshape(n_z * shard_rows, 2 * wide)
    weight = lax.all_gather(block, "y").reshape(n_y, n_z, shard_rows, 2 * wide)
    weight, both_grads, terms = early_pass(
        rows_scale, weight, early_rows, low, high, cotangent, filters
    )
    weight = weight.reshape(depth, 2 * wide)
    terms = terms.reshape(-1, 2 * wide)
    reduced = lax.psum_scatter(terms, "y", scatter_dimension=0, tiled=True)
    reduced = reduced.reshape(n_z, shard_rows + EXTRA, 2 * wide)
    partial = lax.dot_general(
        both_grads, weight, contract_last, preferred_element_type=jnp.float32
    ).astype(jnp.bfloat16)
    cut = depth // 2
    kept = pick(first_c, partial[:, :cut], partial[:, cut:])
    given = pick(first_c, partial[:, cut:], partial[:, :cut])
    chip = kept.astype(jnp.float32) + swapped(given, "c").astype(jnp.float32)
    chip = chip.astype(jnp.bfloat16)
    chip = chip.reshape(2, n_x, row_count // n_x, cut)
    chip = jnp.stack([pick(first_z, chip[0], chip[1]), pick(first_z, chip[1], chip[0])])
    spread = lax.all_to_all(
        chip.reshape(2 * n_x, row_count // n_x, cut), ("zb", "x"), 0, 0, tiled=True
    )
    late_here, late_sent = late_pass(weight, late_rows, low, high, filters)
    spread, late_here, late_sent = lax.optimization_barrier(
        (spread, late_here, late_sent)
    )
    own = jnp.sum(spread.astype(jnp.float32), axis=0).astype(jnp.bfloat16)
    copies = jnp.broadcast_to(own[None], (n_x, *own.shape))
    finished = lax.all_to_all(copies, "x", 0, 0, tiled=True).reshape(row_count, cut)
    late_there = swapped(late_sent, "zb")

    reduced, finished, late_there = lax.optimization_barrier(
        (reduced, finished, late_there)
    )
    pieces = lax.all_to_all(reduced, Z, 0, 0, tiled=True)
    pieces = pieces.reshape(2, 2, shard_rows + EXTRA, 2 * wide).astype(jnp.float32)
    pieces = jnp.sum(pieces, axis=0)
    taps = pieces[:, shard_rows : shard_rows + 3] + pieces[:, shard_rows + 3 : shard_rows + 6]
    pieces = pieces[:, :shard_rows]

    def both(mine, other):
        return joined(pick(first_z, mine, other), pick(first_z, other, mine))

    beside = swapped(finished, "c")
    early_grad = pick(
        first_c,
        jnp.concatenate([finished, beside], axis=1),
        jnp.concatenate([beside, finished], axis=1),
    )
    late_hidden = both(late_here, late_there)
    return (
        late_hidden,
        early_grad,
        gate_grad_sum + joined(pieces[0, :, :wide], pieces[1, :, :wide]),
        up_grad_sum + joined(pieces[0, :, wide:], pieces[1, :, wide:]),
        gate_taps_sum + joined(taps[0, :, :wide], taps[1, :, :wide]),
        up_taps_sum + joined(taps[0, :, wide:], taps[1, :, wide:]),
    )


def solution(mesh):
    split = Mesh(
        mesh.devices.reshape(mesh.shape["rep"], 2, 2, 8, 4, 2),
        ("rep", "zp", "zb", "y", "x", "c"),
    )
    placed = (
        P(REP_FS, None),
        P(REP_FS, None),
        P(REP_FS, TP),
        P(FS, TP),
        P(FS, TP),
        P(None, TP),
        P(None, TP),
        P(REP_FS, TP),
        P(REP_FS, TP),
        P("rep", TP),
        P("rep", TP),
    )
    return jax.shard_map(
        per_device,
        mesh=split,
        in_specs=placed,
        out_specs=(
            P(REP_FS, TP),
            P(REP_FS, None),
            P(REP_FS, TP),
            P(REP_FS, TP),
            P("rep", TP),
            P("rep", TP),
        ),
        check_vma=False,
    )
```

```python
import functools
import math

import jax
import jax.numpy as jnp
from jax import lax
from jax.experimental import pallas as pl
from jax.experimental.pallas import tpu as pltpu
from jax.sharding import Mesh
from jax.sharding import PartitionSpec as P

Z = ("zp", "zb")
FS = ("zp", "zb", "y")
REP_FS = ("rep", "zp", "zb", "y")
TP = ("x", "c")
EXTRA = 8

contract_last = (((1,), (1,)), ((), ()))
contract_first = (((0,), (0,)), ((), ()))


def swapped(values, axis):
    return lax.ppermute(values, axis, [(0, 1), (1, 0)])


def pick(flag, first, second):
    return jnp.where(flag, first, second)


def moved(values, by):
    length = values.shape[0]
    at = lax.broadcasted_iota(jnp.int32, values.shape, 0)
    turned = pltpu.roll(values, by % length, 0)
    inside = at >= by if by > 0 else at < length + by
    return jnp.where(inside, turned, 0.0)


def early_kernel(
    scale,
    gathered,
    own_in,
    low_in,
    high_in,
    cotangent_in,
    filters_in,
    weight_out,
    grads_out,
    terms_out,
    weight,
    grads,
    terms,
    own,
    other,
    cotangent,
    filters,
    in_sems,
    out_sems,
):
    n_y, n_z, shard_rows, columns = gathered.shape
    length = own.shape[0]
    cut = length // 2
    wide = columns // 2
    span = n_y * shard_rows
    fetches = [
        pltpu.make_async_copy(gathered.at[:, z], weight.at[z], in_sems.at[z])
        for z in range(n_z)
    ]
    pairs = (
        (own_in, own),
        (filters_in, filters),
        (cotangent_in, cotangent),
        (low_in.at[:cut], other.at[:cut]),
        (high_in.at[:cut], other.at[cut:]),
    )
    fetches += [
        pltpu.make_async_copy(source, target, in_sems.at[n_z + at])
        for at, (source, target) in enumerate(pairs)
    ]
    blocks, mine, later = fetches[:n_z], fetches[n_z], fetches[n_z + 1 :]
    mine.start()
    for fetch in blocks + later:
        fetch.start()
    first_pre = jnp.zeros((length, columns), jnp.float32)
    mine.wait()
    for z, fetch in enumerate(blocks):
        fetch.wait()
        first_pre = first_pre + jnp.dot(
            own[:, z * span : (z + 1) * span],
            weight[z].reshape(span, columns),
            preferred_element_type=jnp.float32,
        )
    for fetch in later:
        fetch.wait()
    first, second, third = filters[0:1, :], filters[1:2, :], filters[2:3, :]
    slope = math.sqrt(2.0 / math.pi)
    sums = [jnp.zeros((1, columns), jnp.float32) for _ in range(3)]
    stores = [pltpu.make_async_copy(weight, weight_out, out_sems.at[0])]
    stores[0].start()
    for part, rows in enumerate((own, other)):
        pre = first_pre
        if part:
            pre = jnp.dot(
                rows[...],
                weight[...].reshape(n_z * span, columns),
                preferred_element_type=jnp.float32,
            )
        pre = pre.astype(jnp.bfloat16).astype(jnp.float32)
        one_back, two_back = moved(pre, 1), moved(pre, 2)
        mixed = first * two_back + second * one_back + third * pre
        gate, up = mixed[:, :wide], mixed[:, wide:]
        square = gate * gate
        bend = jnp.tanh(slope * (gate + 0.044715 * (square * gate)))
        side = 0.5 * (1.0 + bend)
        active = gate * side
        rise = side + 0.5 * gate * (1.0 - bend * bend) * (
            slope * (1.0 + (3 * 0.044715) * square)
        )
        given = cotangent[part].astype(jnp.float32)
        back = jnp.concatenate([given * up * rise, given * active], axis=1)
        for tap, source in enumerate((two_back, one_back, pre)):
            sums[tap] = sums[tap] + jnp.sum(back * source, axis=0, keepdims=True)
        full = third * back + second * moved(back, -1) + first * moved(back, -2)
        grads[part * length : (part + 1) * length, :] = full.astype(jnp.bfloat16)
    stores.append(pltpu.make_async_copy(grads, grads_out, out_sems.at[1]))
    stores[1].start()
    taps = [scale * value for value in sums]
    high = [value.astype(jnp.bfloat16).astype(jnp.float32) for value in taps]
    blank = jnp.zeros((terms.shape[2] - shard_rows - 6, columns), jnp.float32)
    extra = high + [value - top for value, top in zip(taps, high)] + [blank]
    extra = jnp.concatenate(extra).astype(jnp.bfloat16)
    for z in range(n_z):
        term = sum(
            lax.dot_general(
                rows[:, z * span : (z + 1) * span],
                grads[part * length : (part + 1) * length, :],
                contract_first,
                preferred_element_type=jnp.float32,
            )
            for part, rows in enumerate((own, other))
        )
        term = (term * scale).astype(jnp.bfloat16)
        for y in range(n_y):
            terms[z, y, :shard_rows] = term[y * shard_rows : (y + 1) * shard_rows]
            terms[z, y, shard_rows:] = extra
        store = pltpu.make_async_copy(
            terms.at[z], terms_out.at[:, z], out_sems.at[2 + z]
        )
        store.start()
        stores.append(store)
    for store in stores:
        store.wait()


def early_pass(scale, gathered, own, low, high, cotangent, filters):
    n_y, n_z, shard_rows, columns = gathered.shape
    length, depth = own.shape
    apart = pl.BlockSpec(memory_space=pltpu.HBM)
    ordered = (n_z, n_y, shard_rows, columns)
    return pl.pallas_call(
        functools.partial(early_kernel, scale),
        out_shape=(
            jax.ShapeDtypeStruct(ordered, jnp.bfloat16),
            jax.ShapeDtypeStruct((2 * length, columns), jnp.bfloat16),
            jax.ShapeDtypeStruct((n_y, n_z, shard_rows + EXTRA, columns), jnp.bfloat16),
        ),
        in_specs=[apart] * 6,
        out_specs=(apart,) * 3,
        scratch_shapes=[
            pltpu.VMEM(ordered, jnp.bfloat16),
            pltpu.VMEM((2 * length, columns), jnp.bfloat16),
            pltpu.VMEM((n_z, n_y, shard_rows + EXTRA, columns), jnp.bfloat16),
            pltpu.VMEM(own.shape, jnp.bfloat16),
            pltpu.VMEM(own.shape, jnp.bfloat16),
            pltpu.VMEM(cotangent.shape, jnp.bfloat16),
            pltpu.VMEM((8, columns), jnp.float32),
            pltpu.SemaphoreType.DMA((n_z + 5,)),
            pltpu.SemaphoreType.DMA((2 + n_z,)),
        ],
        compiler_params=pltpu.CompilerParams(vmem_limit_bytes=57 * 1024 * 1024),
        cost_estimate=pl.CostEstimate(
            flops=8 * length * depth * columns,
            bytes_accessed=6 * depth * columns + 4 * length * depth,
            transcendentals=length * columns,
        ),
        name="early_pass",
    )(gathered, own, low, high, cotangent, filters)


def late_kernel(
    weight_in,
    own_in,
    low_in,
    high_in,
    filters_in,
    mine,
    theirs,
    weight,
    own,
    other,
    filters,
    in_sems,
):
    length, wide = mine.shape
    cut = length // 2
    pairs = (
        (own_in, own),
        (weight_in, weight),
        (filters_in, filters),
        (low_in.at[cut:], other.at[:cut]),
        (high_in.at[cut:], other.at[cut:]),
    )
    fetches = [
        pltpu.make_async_copy(source, target, in_sems.at[at])
        for at, (source, target) in enumerate(pairs)
    ]
    for fetch in fetches:
        fetch.start()
    for fetch in fetches:
        fetch.wait()
    first, second, third = filters[0:1, :], filters[1:2, :], filters[2:3, :]
    slope = math.sqrt(2.0 / math.pi)
    for rows, hidden in ((other, theirs), (own, mine)):
        pre = jnp.dot(rows[...], weight[...], preferred_element_type=jnp.float32)
        pre = pre.astype(jnp.bfloat16).astype(jnp.float32)
        mixed = first * moved(pre, 2) + second * moved(pre, 1) + third * pre
        gate, up = mixed[:, :wide], mixed[:, wide:]
        bend = jnp.tanh(slope * (gate + 0.044715 * (gate * gate * gate)))
        hidden[...] = (0.5 * gate * (1.0 + bend) * up).astype(jnp.bfloat16)


def late_pass(weight, own, low, high, filters):
    depth, columns = weight.shape
    length = own.shape[0]
    whole = pl.BlockSpec(memory_space=pltpu.VMEM)
    apart = pl.BlockSpec(memory_space=pltpu.HBM)
    part = jax.ShapeDtypeStruct((length, columns // 2), jnp.bfloat16)
    return pl.pallas_call(
        late_kernel,
        out_shape=(part, part),
        in_specs=[apart] * 5,
        out_specs=(whole, whole),
        scratch_shapes=[
            pltpu.VMEM(weight.shape, jnp.bfloat16),
            pltpu.VMEM(own.shape, jnp.bfloat16),
            pltpu.VMEM(own.shape, jnp.bfloat16),
            pltpu.VMEM(filters.shape, jnp.float32),
            pltpu.SemaphoreType.DMA((5,)),
        ],
        compiler_params=pltpu.CompilerParams(vmem_limit_bytes=58 * 1024 * 1024),
        cost_estimate=pl.CostEstimate(
            flops=4 * length * depth * columns,
            bytes_accessed=2 * depth * columns + 4 * length * depth,
            transcendentals=length * columns,
        ),
        name="late_pass",
    )(weight, own, low, high, filters)


def pack_kernel(gate, up, packed):
    wide = packed.shape[2] // 2
    rows, width = gate.shape
    blank = jnp.zeros((rows, 2 * wide - width), packed.dtype)
    for at, source in ((0, gate), (wide, up)):
        low = source[:, :wide]
        high = jnp.concatenate([source[:, wide:], blank], axis=1)
        for z in range(packed.shape[0]):
            packed[z, :, at : at + wide] = high if z % 2 else low


def packed_halves(gate, up, wide, count):
    whole = pl.BlockSpec(memory_space=pltpu.VMEM)
    return pl.pallas_call(
        pack_kernel,
        out_shape=jax.ShapeDtypeStruct((count, gate.shape[0], 2 * wide), gate.dtype),
        in_specs=[whole] * 2,
        out_specs=whole,
        compiler_params=pltpu.CompilerParams(vmem_limit_bytes=4 * 1024 * 1024),
        name="pack_halves",
    )(gate, up)


def closing_kernel(pieces, gate, up, gate_taps, up_taps, *outs):
    wide = pieces.shape[2] // 2
    shard_rows, width = gate.shape
    rest = width - wide
    sums = [
        pieces[side].astype(jnp.float32) + pieces[2 + side].astype(jnp.float32)
        for side in (0, 1)
    ]
    for source, taps, out, taps_out, at in (
        (gate, gate_taps, outs[0], outs[2], 0),
        (up, up_taps, outs[1], outs[3], wide),
    ):
        for total, start, count in ((sums[0], 0, wide), (sums[1], wide, rest)):
            part = total[:, at : at + count]
            columns = slice(start, start + count)
            out[:, columns] = source[:, columns] + part[:shard_rows]
            extra = part[shard_rows:]
            taps_out[:, columns] = taps[:, columns] + (extra[:3] + extra[3:6])


def closing(pieces, *sums):
    whole = pl.BlockSpec(memory_space=pltpu.VMEM)
    return pl.pallas_call(
        closing_kernel,
        out_shape=tuple(jax.ShapeDtypeStruct(a.shape, a.dtype) for a in sums),
        in_specs=[whole] * 5,
        out_specs=(whole,) * 4,
        compiler_params=pltpu.CompilerParams(vmem_limit_bytes=4 * 1024 * 1024),
        name="closing",
    )(pieces, *sums)


def per_device(
    late_rows,
    early_rows,
    hidden_cot,
    gate_weight,
    up_weight,
    gate_taps,
    up_taps,
    gate_grad_sum,
    up_grad_sum,
    gate_taps_sum,
    up_taps_sum,
):
    row_count, depth = late_rows.shape
    shard_rows, width_local = gate_weight.shape
    wide = -(-width_local // 256) * 128
    rest = width_local - wide
    n_z = lax.axis_size("zp") * lax.axis_size("zb")
    n_y = lax.axis_size("y")
    n_x = lax.axis_size("x")
    zb = lax.axis_index("zb")
    first_z = zb == 0
    first_c = lax.axis_index("c") == 0
    rows_scale = (row_count * n_z * n_y) ** (-0.5)

    def low_high(array):
        edges = [(0, 0)] * (array.ndim - 1)
        return array[..., :wide], jnp.pad(array[..., wide:], edges + [(0, wide - rest)])

    def halves(array):
        low, high = low_high(array)
        return pick(first_z, low, high), pick(first_z, high, low)

    def joined(low, high):
        return jnp.concatenate([low, high[..., :rest]], axis=-1)

    for_z = packed_halves(gate_weight, up_weight, wide, n_z)
    block = lax.all_to_all(for_z, Z, 0, 0, tiled=True)
    half = row_count // 2
    sent = jnp.concatenate(
        [pick(first_c, rows[:half], rows[half:]) for rows in (early_rows, late_rows)]
    )
    here = swapped(sent, "zb")
    there = swapped(here, "c")
    low, high = pick(first_c, here, there), pick(first_c, there, here)
    cot_mine, cot_other = halves(hidden_cot)
    cotangent = jnp.stack([cot_mine, swapped(cot_other, "zb")])
    filters = jnp.concatenate([halves(gate_taps)[0], halves(up_taps)[0]], axis=1)
    filters = jnp.pad(filters.astype(jnp.float32), [(0, 5), (0, 0)])

    block = block.reshape(n_z * shard_rows, 2 * wide)
    weight = lax.all_gather(block, "y").reshape(n_y, n_z, shard_rows, 2 * wide)
    weight, both_grads, terms = early_pass(
        rows_scale, weight, early_rows, low, high, cotangent, filters
    )
    weight = weight.reshape(depth, 2 * wide)
    terms = terms.reshape(-1, 2 * wide)
    reduced = lax.psum_scatter(terms, "y", scatter_dimension=0, tiled=True)
    reduced = reduced.reshape(n_z, shard_rows + EXTRA, 2 * wide)
    partial = lax.dot_general(
        both_grads, weight, contract_last, preferred_element_type=jnp.float32
    ).astype(jnp.bfloat16)
    cut = depth // 2
    kept = pick(first_c, partial[:, :cut], partial[:, cut:])
    given = pick(first_c, partial[:, cut:], partial[:, :cut])
    chip = kept.astype(jnp.float32) + swapped(given, "c").astype(jnp.float32)
    chip = chip.astype(jnp.bfloat16)
    chip = chip.reshape(2, n_x, row_count // n_x, cut)
    chip = jnp.stack([pick(first_z, chip[0], chip[1]), pick(first_z, chip[1], chip[0])])
    spread = lax.all_to_all(
        chip.reshape(2 * n_x, row_count // n_x, cut), ("zb", "x"), 0, 0, tiled=True
    )
    late_here, late_sent = late_pass(weight, late_rows, low, high, filters)
    spread, late_here, late_sent = lax.optimization_barrier(
        (spread, late_here, late_sent)
    )
    own = jnp.sum(spread.astype(jnp.float32), axis=0).astype(jnp.bfloat16)
    copies = jnp.broadcast_to(own[None], (n_x, *own.shape))
    finished = lax.all_to_all(copies, "x", 0, 0, tiled=True).reshape(row_count, cut)
    late_there = swapped(late_sent, "zb")

    reduced, finished, late_there = lax.optimization_barrier(
        (reduced, finished, late_there)
    )
    pieces = lax.all_to_all(reduced, Z, 0, 0, tiled=True)
    closed = closing(pieces, gate_grad_sum, up_grad_sum, gate_taps_sum, up_taps_sum)

    def both(mine, other):
        return joined(pick(first_z, mine, other), pick(first_z, other, mine))

    beside = swapped(finished, "c")
    early_grad = pick(
        first_c,
        jnp.concatenate([finished, beside], axis=1),
        jnp.concatenate([beside, finished], axis=1),
    )
    late_hidden = both(late_here, late_there)
    return (
        late_hidden,
        early_grad,
        *closed,
    )


def solution(mesh):
    split = Mesh(
        mesh.devices.reshape(mesh.shape["rep"], 2, 2, 8, 4, 2),
        ("rep", "zp", "zb", "y", "x", "c"),
    )
    placed = (
        P(REP_FS, None),
        P(REP_FS, None),
        P(REP_FS, TP),
        P(FS, TP),
        P(FS, TP),
        P(None, TP),
        P(None, TP),
        P(REP_FS, TP),
        P(REP_FS, TP),
        P("rep", TP),
        P("rep", TP),
    )
    return jax.shard_map(
        per_device,
        mesh=split,
        in_specs=placed,
        out_specs=(
            P(REP_FS, TP),
            P(REP_FS, None),
            P(REP_FS, TP),
            P(REP_FS, TP),
            P("rep", TP),
            P("rep", TP),
        ),
        check_vma=False,
    )
```

```python
import functools
import math

import jax
import jax.numpy as jnp
from jax import lax
from jax.experimental import pallas as pl
from jax.experimental.pallas import tpu as pltpu
from jax.sharding import Mesh
from jax.sharding import PartitionSpec as P

Z = ("zp", "zb")
FS = ("zp", "zb", "y")
REP_FS = ("rep", "zp", "zb", "y")
TP = ("x", "c")
EXTRA = 8

contract_last = (((1,), (1,)), ((), ()))
contract_first = (((0,), (0,)), ((), ()))


def swapped(values, axis):
    return lax.ppermute(values, axis, [(0, 1), (1, 0)])


def pick(flag, first, second):
    return jnp.where(flag, first, second)


def moved(values, by):
    length = values.shape[0]
    at = lax.broadcasted_iota(jnp.int32, values.shape, 0)
    turned = pltpu.roll(values, by % length, 0)
    inside = at >= by if by > 0 else at < length + by
    return jnp.where(inside, turned, 0.0)


def early_kernel(
    scale,
    gathered,
    own_in,
    low_in,
    high_in,
    cotangent_in,
    filters_in,
    weight_out,
    grads_out,
    terms_out,
    weight,
    grads,
    terms,
    own,
    other,
    cotangent,
    filters,
    in_sems,
    out_sems,
):
    n_y, n_z, shard_rows, columns = gathered.shape
    length = own.shape[0]
    cut = length // 2
    wide = columns // 2
    span = n_y * shard_rows
    fetches = [
        pltpu.make_async_copy(gathered.at[:, z], weight.at[z], in_sems.at[z])
        for z in range(n_z)
    ]
    pairs = (
        (own_in, own),
        (filters_in, filters),
        (cotangent_in, cotangent),
        (low_in.at[:cut], other.at[:cut]),
        (high_in.at[:cut], other.at[cut:]),
    )
    fetches += [
        pltpu.make_async_copy(source, target, in_sems.at[n_z + at])
        for at, (source, target) in enumerate(pairs)
    ]
    blocks, mine, later = fetches[:n_z], fetches[n_z], fetches[n_z + 1 :]
    mine.start()
    for fetch in blocks + later:
        fetch.start()
    mine.wait()
    for fetch in blocks:
        fetch.wait()
    first_pre = jnp.dot(
        own[...],
        weight[...].reshape(n_z * span, columns),
        preferred_element_type=jnp.float32,
    )
    for fetch in later:
        fetch.wait()
    first, second, third = filters[0:1, :], filters[1:2, :], filters[2:3, :]
    slope = math.sqrt(2.0 / math.pi)
    sums = [jnp.zeros((1, columns), jnp.float32) for _ in range(3)]
    stores = [pltpu.make_async_copy(weight, weight_out, out_sems.at[0])]
    stores[0].start()
    for part, rows in enumerate((own, other)):
        pre = first_pre
        if part:
            pre = jnp.dot(
                rows[...],
                weight[...].reshape(n_z * span, columns),
                preferred_element_type=jnp.float32,
            )
        pre = pre.astype(jnp.bfloat16).astype(jnp.float32)
        one_back, two_back = moved(pre, 1), moved(pre, 2)
        mixed = first * two_back + second * one_back + third * pre
        gate, up = mixed[:, :wide], mixed[:, wide:]
        square = gate * gate
        bend = jnp.tanh(slope * (gate + 0.044715 * (square * gate)))
        side = 0.5 * (1.0 + bend)
        active = gate * side
        rise = side + 0.5 * gate * (1.0 - bend * bend) * (
            slope * (1.0 + (3 * 0.044715) * square)
        )
        given = cotangent[part].astype(jnp.float32)
        back = jnp.concatenate([given * up * rise, given * active], axis=1)
        for tap, source in enumerate((two_back, one_back, pre)):
            sums[tap] = sums[tap] + jnp.sum(back * source, axis=0, keepdims=True)
        full = third * back + second * moved(back, -1) + first * moved(back, -2)
        grads[part * length : (part + 1) * length, :] = full.astype(jnp.bfloat16)
    stores.append(pltpu.make_async_copy(grads, grads_out, out_sems.at[1]))
    stores[1].start()
    taps = [scale * value for value in sums]
    high = [value.astype(jnp.bfloat16).astype(jnp.float32) for value in taps]
    blank = jnp.zeros((terms.shape[2] - shard_rows - 6, columns), jnp.float32)
    extra = high + [value - top for value, top in zip(taps, high)] + [blank]
    extra = jnp.concatenate(extra).astype(jnp.bfloat16)
    for z in range(n_z):
        term = sum(
            lax.dot_general(
                rows[:, z * span : (z + 1) * span],
                grads[part * length : (part + 1) * length, :],
                contract_first,
                preferred_element_type=jnp.float32,
            )
            for part, rows in enumerate((own, other))
        )
        term = (term * scale).astype(jnp.bfloat16)
        for y in range(n_y):
            terms[z, y, :shard_rows] = term[y * shard_rows : (y + 1) * shard_rows]
            terms[z, y, shard_rows:] = extra
        store = pltpu.make_async_copy(
            terms.at[z], terms_out.at[:, z], out_sems.at[2 + z]
        )
        store.start()
        stores.append(store)
    for store in stores:
        store.wait()


def early_pass(scale, gathered, own, low, high, cotangent, filters):
    n_y, n_z, shard_rows, columns = gathered.shape
    length, depth = own.shape
    apart = pl.BlockSpec(memory_space=pltpu.HBM)
    ordered = (n_z, n_y, shard_rows, columns)
    return pl.pallas_call(
        functools.partial(early_kernel, scale),
        out_shape=(
            jax.ShapeDtypeStruct(ordered, jnp.bfloat16),
            jax.ShapeDtypeStruct((2 * length, columns), jnp.bfloat16),
            jax.ShapeDtypeStruct((n_y, n_z, shard_rows + EXTRA, columns), jnp.bfloat16),
        ),
        in_specs=[apart] * 6,
        out_specs=(apart,) * 3,
        scratch_shapes=[
            pltpu.VMEM(ordered, jnp.bfloat16),
            pltpu.VMEM((2 * length, columns), jnp.bfloat16),
            pltpu.VMEM((n_z, n_y, shard_rows + EXTRA, columns), jnp.bfloat16),
            pltpu.VMEM(own.shape, jnp.bfloat16),
            pltpu.VMEM(own.shape, jnp.bfloat16),
            pltpu.VMEM(cotangent.shape, jnp.bfloat16),
            pltpu.VMEM((8, columns), jnp.float32),
            pltpu.SemaphoreType.DMA((n_z + 5,)),
            pltpu.SemaphoreType.DMA((2 + n_z,)),
        ],
        compiler_params=pltpu.CompilerParams(vmem_limit_bytes=57 * 1024 * 1024),
        cost_estimate=pl.CostEstimate(
            flops=8 * length * depth * columns,
            bytes_accessed=6 * depth * columns + 4 * length * depth,
            transcendentals=length * columns,
        ),
        name="early_pass",
    )(gathered, own, low, high, cotangent, filters)


def late_kernel(
    weight_in,
    own_in,
    low_in,
    high_in,
    filters_in,
    mine,
    theirs,
    weight,
    own,
    other,
    filters,
    in_sems,
):
    length, wide = mine.shape
    cut = length // 2
    pairs = (
        (own_in, own),
        (weight_in, weight),
        (filters_in, filters),
        (low_in.at[cut:], other.at[:cut]),
        (high_in.at[cut:], other.at[cut:]),
    )
    fetches = [
        pltpu.make_async_copy(source, target, in_sems.at[at])
        for at, (source, target) in enumerate(pairs)
    ]
    for fetch in fetches:
        fetch.start()
    for fetch in fetches:
        fetch.wait()
    first, second, third = filters[0:1, :], filters[1:2, :], filters[2:3, :]
    slope = math.sqrt(2.0 / math.pi)
    for rows, hidden in ((other, theirs), (own, mine)):
        pre = jnp.dot(rows[...], weight[...], preferred_element_type=jnp.float32)
        pre = pre.astype(jnp.bfloat16).astype(jnp.float32)
        mixed = first * moved(pre, 2) + second * moved(pre, 1) + third * pre
        gate, up = mixed[:, :wide], mixed[:, wide:]
        bend = jnp.tanh(slope * (gate + 0.044715 * (gate * gate * gate)))
        hidden[...] = (0.5 * gate * (1.0 + bend) * up).astype(jnp.bfloat16)


def late_pass(weight, own, low, high, filters):
    depth, columns = weight.shape
    length = own.shape[0]
    whole = pl.BlockSpec(memory_space=pltpu.VMEM)
    apart = pl.BlockSpec(memory_space=pltpu.HBM)
    part = jax.ShapeDtypeStruct((length, columns // 2), jnp.bfloat16)
    return pl.pallas_call(
        late_kernel,
        out_shape=(part, part),
        in_specs=[apart] * 5,
        out_specs=(whole, whole),
        scratch_shapes=[
            pltpu.VMEM(weight.shape, jnp.bfloat16),
            pltpu.VMEM(own.shape, jnp.bfloat16),
            pltpu.VMEM(own.shape, jnp.bfloat16),
            pltpu.VMEM(filters.shape, jnp.float32),
            pltpu.SemaphoreType.DMA((5,)),
        ],
        compiler_params=pltpu.CompilerParams(vmem_limit_bytes=58 * 1024 * 1024),
        cost_estimate=pl.CostEstimate(
            flops=4 * length * depth * columns,
            bytes_accessed=2 * depth * columns + 4 * length * depth,
            transcendentals=length * columns,
        ),
        name="late_pass",
    )(weight, own, low, high, filters)


def pack_kernel(gate, up, packed):
    wide = packed.shape[2] // 2
    rows, width = gate.shape
    blank = jnp.zeros((rows, 2 * wide - width), packed.dtype)
    for at, source in ((0, gate), (wide, up)):
        low = source[:, :wide]
        high = jnp.concatenate([source[:, wide:], blank], axis=1)
        for z in range(packed.shape[0]):
            packed[z, :, at : at + wide] = high if z % 2 else low


def packed_halves(gate, up, wide, count):
    whole = pl.BlockSpec(memory_space=pltpu.VMEM)
    return pl.pallas_call(
        pack_kernel,
        out_shape=jax.ShapeDtypeStruct((count, gate.shape[0], 2 * wide), gate.dtype),
        in_specs=[whole] * 2,
        out_specs=whole,
        compiler_params=pltpu.CompilerParams(vmem_limit_bytes=4 * 1024 * 1024),
        name="pack_halves",
    )(gate, up)


def closing_kernel(pieces, gate, up, gate_taps, up_taps, *outs):
    wide = pieces.shape[2] // 2
    shard_rows, width = gate.shape
    rest = width - wide
    sums = [
        pieces[side].astype(jnp.float32) + pieces[2 + side].astype(jnp.float32)
        for side in (0, 1)
    ]
    for source, taps, out, taps_out, at in (
        (gate, gate_taps, outs[0], outs[2], 0),
        (up, up_taps, outs[1], outs[3], wide),
    ):
        for total, start, count in ((sums[0], 0, wide), (sums[1], wide, rest)):
            part = total[:, at : at + count]
            columns = slice(start, start + count)
            out[:, columns] = source[:, columns] + part[:shard_rows]
            extra = part[shard_rows:]
            taps_out[:, columns] = taps[:, columns] + (extra[:3] + extra[3:6])


def closing(pieces, *sums):
    whole = pl.BlockSpec(memory_space=pltpu.VMEM)
    return pl.pallas_call(
        closing_kernel,
        out_shape=tuple(jax.ShapeDtypeStruct(a.shape, a.dtype) for a in sums),
        in_specs=[whole] * 5,
        out_specs=(whole,) * 4,
        compiler_params=pltpu.CompilerParams(vmem_limit_bytes=4 * 1024 * 1024),
        name="closing",
    )(pieces, *sums)


def per_device(
    late_rows,
    early_rows,
    hidden_cot,
    gate_weight,
    up_weight,
    gate_taps,
    up_taps,
    gate_grad_sum,
    up_grad_sum,
    gate_taps_sum,
    up_taps_sum,
):
    row_count, depth = late_rows.shape
    shard_rows, width_local = gate_weight.shape
    wide = -(-width_local // 256) * 128
    rest = width_local - wide
    n_z = lax.axis_size("zp") * lax.axis_size("zb")
    n_y = lax.axis_size("y")
    n_x = lax.axis_size("x")
    zb = lax.axis_index("zb")
    first_z = zb == 0
    first_c = lax.axis_index("c") == 0
    rows_scale = (row_count * n_z * n_y) ** (-0.5)

    def low_high(array):
        edges = [(0, 0)] * (array.ndim - 1)
        return array[..., :wide], jnp.pad(array[..., wide:], edges + [(0, wide - rest)])

    def halves(array):
        low, high = low_high(array)
        return pick(first_z, low, high), pick(first_z, high, low)

    def joined(low, high):
        return jnp.concatenate([low, high[..., :rest]], axis=-1)

    for_z = packed_halves(gate_weight, up_weight, wide, n_z)
    block = lax.all_to_all(for_z, Z, 0, 0, tiled=True)
    half = row_count // 2
    sent = jnp.concatenate(
        [pick(first_c, rows[:half], rows[half:]) for rows in (early_rows, late_rows)]
    )
    here = swapped(sent, "zb")
    there = swapped(here, "c")
    low, high = pick(first_c, here, there), pick(first_c, there, here)
    cot_mine, cot_other = halves(hidden_cot)
    cotangent = jnp.stack([cot_mine, swapped(cot_other, "zb")])
    filters = jnp.concatenate([halves(gate_taps)[0], halves(up_taps)[0]], axis=1)
    filters = jnp.pad(filters.astype(jnp.float32), [(0, 5), (0, 0)])

    block = block.reshape(n_z * shard_rows, 2 * wide)
    weight = lax.all_gather(block, "y").reshape(n_y, n_z, shard_rows, 2 * wide)
    weight, both_grads, terms = early_pass(
        rows_scale, weight, early_rows, low, high, cotangent, filters
    )
    weight = weight.reshape(depth, 2 * wide)
    terms = terms.reshape(-1, 2 * wide)
    reduced = lax.psum_scatter(terms, "y", scatter_dimension=0, tiled=True)
    reduced = reduced.reshape(n_z, shard_rows + EXTRA, 2 * wide)
    partial = lax.dot_general(
        both_grads, weight, contract_last, preferred_element_type=jnp.float32
    ).astype(jnp.bfloat16)
    cut = depth // 2
    kept = pick(first_c, partial[:, :cut], partial[:, cut:])
    given = pick(first_c, partial[:, cut:], partial[:, :cut])
    chip = kept.astype(jnp.float32) + swapped(given, "c").astype(jnp.float32)
    chip = chip.astype(jnp.bfloat16)
    chip = chip.reshape(2, n_x, row_count // n_x, cut)
    chip = jnp.stack([pick(first_z, chip[0], chip[1]), pick(first_z, chip[1], chip[0])])
    spread = lax.all_to_all(
        chip.reshape(2 * n_x, row_count // n_x, cut), ("zb", "x"), 0, 0, tiled=True
    )
    late_here, late_sent = late_pass(weight, late_rows, low, high, filters)
    spread, late_here, late_sent = lax.optimization_barrier(
        (spread, late_here, late_sent)
    )
    own = jnp.sum(spread.astype(jnp.float32), axis=0).astype(jnp.bfloat16)
    copies = jnp.broadcast_to(own[None], (n_x, *own.shape))
    finished = lax.all_to_all(copies, "x", 0, 0, tiled=True).reshape(row_count, cut)
    late_there = swapped(late_sent, "zb")

    beside = swapped(finished, "c")
    reduced, finished, beside, late_there = lax.optimization_barrier(
        (reduced, finished, beside, late_there)
    )
    pieces = lax.all_to_all(reduced, Z, 0, 0, tiled=True)
    closed = closing(pieces, gate_grad_sum, up_grad_sum, gate_taps_sum, up_taps_sum)

    def both(mine, other):
        return joined(pick(first_z, mine, other), pick(first_z, other, mine))

    early_grad = pick(
        first_c,
        jnp.concatenate([finished, beside], axis=1),
        jnp.concatenate([beside, finished], axis=1),
    )
    late_hidden = both(late_here, late_there)
    return (
        late_hidden,
        early_grad,
        *closed,
    )


def solution(mesh):
    split = Mesh(
        mesh.devices.reshape(mesh.shape["rep"], 2, 2, 8, 4, 2),
        ("rep", "zp", "zb", "y", "x", "c"),
    )
    placed = (
        P(REP_FS, None),
        P(REP_FS, None),
        P(REP_FS, TP),
        P(FS, TP),
        P(FS, TP),
        P(None, TP),
        P(None, TP),
        P(REP_FS, TP),
        P(REP_FS, TP),
        P("rep", TP),
        P("rep", TP),
    )
    return jax.shard_map(
        per_device,
        mesh=split,
        in_specs=placed,
        out_specs=(
            P(REP_FS, TP),
            P(REP_FS, None),
            P(REP_FS, TP),
            P(REP_FS, TP),
            P("rep", TP),
            P("rep", TP),
        ),
        check_vma=False,
    )
```
